32 devices in a mesh: kv: 8 (over z, y), tp: 4 (over x, core).
Axes of the slice: x: 2, y: 2, z: 4, core: 2. Of those that a mesh axis runs over, the one named last changes fastest.
Arguments:
- activations: bfloat16 [64, 4096], P(None, ('kv', 'tp')), may hold values from -60 to 60
- mixer_gain: bfloat16 [4096], P(('kv', 'tp')), may hold values from 0.099609375 to 1.8984375
- channel_gain: bfloat16 [4096], P(('kv', 'tp')), may hold values from 0.099609375 to 1.8984375
- query_weight: bfloat16 [4096, 4096], P('kv', 'tp'), may hold values from -0.09375 to 0.09375
- key_weight: bfloat16 [4096, 4096], P('kv', 'tp'), may hold values from -0.09375 to 0.09375
- value_weight: bfloat16 [4096, 8192], P('kv', 'tp'), may hold values from -0.09375 to 0.09375
- gate_weight: bfloat16 [4096, 8192], P('kv', 'tp'), may hold values from -0.09375 to 0.09375
- output_weight: bfloat16 [8192, 4096], P('tp', 'kv'), may hold values from -0.1875 to 0.1875
- up_weight: bfloat16 [4096, 16384], P('kv', 'tp'), may hold values from -0.09375 to 0.09375
- down_weight: bfloat16 [16384, 4096], P('tp', 'kv'), may hold values from -0.046875 to 0.046875
- state_in: float32 [64, 16, 256, 512], P('kv', 'tp'), may hold values from -0.5 to 0.5
Outputs:
- activations_out: bfloat16 [64, 4096], P(None, ('kv', 'tp'))
- state_out: float32 [64, 16, 256, 512], P('kv', 'tp')
The draws below stay inside these ranges and needn't reach their ends.
All inputs are finite; a program needn't handle non-finite values.
Results may differ from the reference program's by a relative error of at most 0.022.
Values may be sent and summed in bfloat16 or wider, within the bound.
A program may use at most 128 MiB of HBM per device.

```python
import jax
import jax.numpy as jnp
from jax import lax

D = 4096
HEADS = 16
DK = 256
DV = 512
FF = 16384
BATCH = 64
QK = 4096
RV = 8192
N_TP = 4


def draw_activations(key, part):
    base_key, row_key = jax.random.split(key, 2)
    columns = jnp.exp(jnp.linspace(0.0, jnp.log(3.0), D, dtype=jnp.float32))
    base = jnp.clip(jax.random.normal(base_key, (BATCH, D), jnp.float32), -5.0, 5.0)
    scales = jnp.exp(jax.random.uniform(row_key, (BATCH, 1), jnp.float32, jnp.log(0.3), jnp.log(3.0)))
    return jnp.clip(base * scales * columns, -60.0, 60.0).astype(jnp.bfloat16)


def level_of(key, extent, shards, least, high):
    factor_of, own = 1.0, jax.random.fold_in(key, 6)
    for axis_at, shards_of in shards:
        heights = jnp.exp(jax.random.uniform(jax.random.fold_in(own, axis_at), (shards_of,), jnp.float32, least / len(shards), high / len(shards)))
        factor_of = factor_of * jnp.repeat(heights, extent[axis_at] // shards_of).reshape([-1 if axis == axis_at else 1 for axis in range(len(extent))])
    return factor_of


def normal_values(own_key, dims, spread, most, pieces=(), kind=jnp.bfloat16):
    values = spread * jax.random.normal(own_key, dims, jnp.float32)
    if pieces:
        values = values * level_of(own_key, dims, pieces, -0.22, 0.18)
    return jnp.clip(values, -most, most).astype(kind)


def setup_inputs(seed: int = 0) -> dict:
    key_list = jax.random.split(jax.random.key(seed), 12)
    activations = draw_activations(jax.random.fold_in(key_list[11], 71), 0)
    mixer_gain = jnp.clip(1.0 + 0.18 * jax.random.normal(key_list[1], (D,), jnp.float32), 0.099609375, 1.8984375).astype(jnp.bfloat16)
    channel_gain = jnp.clip(1.0 + 0.18 * jax.random.normal(key_list[2], (D,), jnp.float32), 0.099609375, 1.8984375).astype(jnp.bfloat16)
    query_weight = normal_values(key_list[3], (D, QK), D ** -0.5, 0.09375, ((0, 8), (1, 4)))
    key_weight = normal_values(key_list[4], (D, QK), D ** -0.5, 0.09375, ((0, 8), (1, 4)))
    value_weight = normal_values(key_list[5], (D, RV), D ** -0.5, 0.09375, ((0, 8), (1, 4)))
    gate_weight = normal_values(key_list[6], (D, RV), D ** -0.5, 0.09375, ((0, 8), (1, 4)))
    output_weight = normal_values(key_list[7], (RV, D), (RV // 8) ** -0.5, 0.1875, ((0, 4), (1, 8)))
    up_weight = normal_values(key_list[8], (D, FF), D ** -0.5, 0.09375, ((0, 8), (1, 4)))
    down_weight = normal_values(key_list[9], (FF, D), FF ** -0.5, 0.046875, ((0, 4), (1, 8)))
    state_in = normal_values(key_list[10], (BATCH, HEADS, DK, DV), 0.06, 0.5, ((0, 8), (1, 4)), jnp.float32)
    return dict(activations=activations, mixer_gain=mixer_gain, channel_gain=channel_gain, query_weight=query_weight, key_weight=key_weight, value_weight=value_weight, gate_weight=gate_weight, output_weight=output_weight, up_weight=up_weight, down_weight=down_weight, state_in=state_in)


EPS = 1e-06

def head_decays(count):
    index = jnp.arange(count, dtype=jnp.float32)
    return 1.0 - 2.0 ** (-1.0 - 6.0 * index / (count - 1))

def summed_blocks(left, right, parts):
    width = left.shape[1] // parts
    total = jnp.zeros((left.shape[0], right.shape[1]), jnp.float32)
    for index in range(parts):
        term = jnp.dot(left[:, index * width:(index + 1) * width], right[index * width:(index + 1) * width], preferred_element_type=jnp.float32)
        total = total + lax.optimization_barrier(term.astype(jnp.bfloat16)).astype(jnp.float32)
    return total

def reference(activations, mixer_gain, channel_gain, query_weight, key_weight, value_weight, gate_weight, output_weight, up_weight, down_weight, state_in):
    stream = activations.astype(jnp.float32)
    scale_rows = lax.rsqrt(lax.optimization_barrier(jnp.sum(stream * stream, axis=1, keepdims=True)) / D + EPS)
    normed = (stream * mixer_gain.astype(jnp.float32)).astype(jnp.bfloat16)
    query = scale_rows * jnp.dot(normed, query_weight, preferred_element_type=jnp.float32)
    key = scale_rows * jnp.dot(normed, key_weight, preferred_element_type=jnp.float32) * DK ** (-0.5)
    value = scale_rows * jnp.dot(normed, value_weight, preferred_element_type=jnp.float32)
    gate = scale_rows * jnp.dot(normed, gate_weight, preferred_element_type=jnp.float32)
    rates = head_decays(HEADS)

    def advance(inputs):
        query_row, key_row, value_row, old_state = inputs
        query_heads = query_row.reshape(HEADS, DK)
        key_heads = key_row.reshape(HEADS, DK)
        value_heads = value_row.reshape(HEADS, DV)
        new_state = rates[:, None, None] * old_state + key_heads[:, :, None] * value_heads[:, None, :]
        output = jnp.einsum('hd,hde->he', query_heads, new_state, precision=lax.Precision.HIGHEST)
        return (new_state, output)
    state_out, retained = lax.map(advance, (query, key, value, state_in))
    retained = retained * lax.rsqrt(lax.optimization_barrier(jnp.mean(retained * retained, axis=2, keepdims=True)) + EPS)
    mixed = (jax.nn.silu(gate) * retained.reshape(retained.shape[0], HEADS * DV)).astype(jnp.bfloat16)
    attention = summed_blocks(mixed, output_weight, N_TP)
    middle = (stream + attention).astype(jnp.bfloat16)
    middle = lax.optimization_barrier(middle).astype(jnp.float32)
    channel_scale = lax.rsqrt(lax.optimization_barrier(jnp.sum(middle * middle, axis=1, keepdims=True)) / D + EPS)
    channel_normed = (middle * channel_gain.astype(jnp.float32)).astype(jnp.bfloat16)
    lifted = channel_scale * jnp.dot(channel_normed, up_weight, preferred_element_type=jnp.float32)
    hidden = jnp.square(jax.nn.relu(lifted)).astype(jnp.bfloat16)
    lowered = summed_blocks(hidden, down_weight, N_TP)
    return ((middle + lowered).astype(jnp.bfloat16), state_out)
```

```python
import functools

import jax
import jax.numpy as jnp
from jax import lax
from jax.experimental import pallas as pl
from jax.experimental.pallas import tpu as pltpu
from jax.sharding import PartitionSpec as P

HEADS = 16
EPS = 1e-06
MESH = pl.DeviceIdType.MESH
F32 = jnp.float32
BF16 = jnp.bfloat16
DMA = pltpu.SemaphoreType.DMA
PAIR = 2
CORES = 2
GAIN_ROWS = 16
WIDTH = 512
LAG_A, LAG_B = 5, 5
LAG_1, LAG_2, LAG_3, LAG_4 = 4, 4, 4, 3


def head_decays(count):
    index = jnp.arange(count, dtype=jnp.float32)
    return 1.0 - 2.0 ** (-1.0 - 6.0 * index / (count - 1))


def put(src, dst, send_sem, recv_sem, where):
    copy = pltpu.make_async_remote_copy(
        src_ref=src,
        dst_ref=dst,
        send_sem=send_sem,
        recv_sem=recv_sem,
        device_id=where,
        device_id_type=MESH,
    )
    copy.start()
    return copy


def tp_gather(buf, tp, n_tp, sems):
    return [
        put(
            buf.at[tp],
            buf.at[tp],
            sems.at[0, d - 1],
            sems.at[1, d - 1],
            {"tp": lax.rem(tp + d, n_tp)},
        )
        for d in range(1, n_tp)
    ]


def tp_scatter(src, dst, tp, n_tp, sems):
    copies = []
    for d in range(1, n_tp):
        peer = lax.rem(tp + d, n_tp)
        copies.append(
            put(src.at[peer], dst.at[d - 1], sems.at[0, d - 1], sems.at[1, d - 1], {"tp": peer})
        )
    return copies


def kv_scatter_small(src, dst, kv, n_kv, sems):
    copies = []
    for d in range(1, n_kv):
        peer = lax.rem(kv + d, n_kv)
        copies.append(
            put(src.at[peer], dst.at[d - 1], sems.at[0, d - 1], sems.at[1, d - 1], {"kv": peer})
        )
    return copies


def own_square_total(squares, sq_src, sq_dst, kv, n_kv, rows, sems):
    for g in range(n_kv):
        sq_src[g] = jnp.broadcast_to(squares[g * rows : (g + 1) * rows], sq_src.shape[1:])
    copies = kv_scatter_small(sq_src, sq_dst, kv, n_kv, sems)

    def finish():
        total = sq_src[kv]
        for d, copy in enumerate(copies):
            copy.wait_recv()
            total = total + sq_dst[d]
        return total[:, :1]

    return copies, finish


class PairScatter:
    def __init__(self, kv, n_kv, rows, part, got, summed, got2, sem_a, sem_b):
        self.n_z = n_kv // PAIR
        self.z, self.y = lax.div(kv, PAIR), lax.rem(kv, PAIR)
        self.rows = rows
        self.part, self.got, self.summed, self.got2 = part, got, summed, got2
        self.sem_a, self.sem_b = sem_a, sem_b
        self.first, self.second = {}, {}

    def start(self, p, value):
        rows = self.rows
        for z in range(self.n_z):
            for y in range(PAIR):
                at = (z * PAIR + y) * rows
                self.part[p, y, z] = value[at : at + rows].astype(BF16)
        other = 1 - self.y
        self.first[p] = put(
            self.part.at[p, other],
            self.got.at[p],
            self.sem_a.at[0, p],
            self.sem_a.at[1, p],
            {"kv": self.z * PAIR + other},
        )

    def middle(self, p):
        self.first[p].wait_recv()
        self.summed[p] = (self.part[p, self.y].astype(F32) + self.got[p].astype(F32)).astype(BF16)
        copies = []
        for d in range(1, self.n_z):
            peer = lax.rem(self.z + d, self.n_z)
            copies.append(
                put(
                    self.summed.at[p, peer],
                    self.got2.at[p, d - 1],
                    self.sem_b.at[0, p, d - 1],
                    self.sem_b.at[1, p, d - 1],
                    {"kv": peer * PAIR + self.y},
                )
            )
        self.second[p] = copies

    def finish(self, p):
        total = self.summed[p, self.z].astype(F32)
        for d, copy in enumerate(self.second[p]):
            copy.wait_recv()
            total = total + self.got2[p, d].astype(F32)
        return total

    def drain(self):
        for p in self.first:
            self.first[p].wait_send()
            for copy in self.second[p]:
                copy.wait_send()


class PairGather:
    def __init__(self, kv, n_kv, buf, sem_z, sem_y):
        self.n_z = n_kv // PAIR
        self.z, self.y = lax.div(kv, PAIR), lax.rem(kv, PAIR)
        self.buf, self.sem_z, self.sem_y = buf, sem_z, sem_y
        self.along, self.across = {}, {}

    def forward(self, p, d):
        z = lax.rem(self.z - d + self.n_z, self.n_z)
        self.across[p].append(
            put(
                self.buf.at[p, z, self.y],
                self.buf.at[p, z, self.y],
                self.sem_y.at[0, p, d],
                self.sem_y.at[1, p, d],
                {"kv": self.z * PAIR + 1 - self.y},
            )
        )

    def start(self, p):
        own = self.buf.at[p, self.z, self.y]
        self.along[p], self.across[p] = [], []
        for d in range(1, self.n_z):
            peer = lax.rem(self.z + d, self.n_z)
            self.along[p].append(
                put(
                    own,
                    own,
                    self.sem_z.at[0, p, d - 1],
                    self.sem_z.at[1, p, d - 1],
                    {"kv": peer * PAIR + self.y},
                )
            )
        self.forward(p, 0)

    def relay(self, p):
        for d, copy in enumerate(self.along[p]):
            copy.wait_recv()
            self.forward(p, d + 1)

    def finish(self, p):
        for copy in self.across[p]:
            copy.wait_recv()
        blocks = [
            self.buf[p, z, y].astype(F32) for z in range(self.n_z) for y in range(PAIR)
        ]
        return jnp.concatenate(blocks, axis=0).astype(BF16)

    def drain(self):
        for p in self.along:
            for copy in self.along[p] + self.across[p]:
                copy.wait_send()


def fused_kernel(sizes, rate_ref, x_hbm, mg_hbm, cg_hbm, *refs):
    n_kv, n_tp, rows, width, dk, dv, heads, dim = sizes
    (qw_hbm, kw_hbm, vw_hbm, gw_hbm, ow_hbm, up_hbm, down_hbm, old_hbm) = refs[:8]
    (out_ref, k_ref, v_ref, held) = refs[8:12]
    (pack, gain_in, qw, kw, vw, gw, ow, up, down) = refs[12:21]
    (part, got, summed, got2, part_u, got_u, summed_u, got2_u) = refs[21:29]
    (sq_src, sq_dst, sq_src2, sq_dst2, mixes, hid, ret, acc) = refs[29:37]
    (pair_own, pair_got, chip, far, mids, ends, got_ends) = refs[37:44]
    (w_sem, s_sem, in_sem, t_sem, sq_sem, sq_sem2) = refs[44:50]
    (sem_a, sem_b, sem_ua, sem_ub, mz_sem, my_sem, hz_sem, hy_sem) = refs[50:58]
    (c_sem, far_sem, f_sem) = refs[58:61]
    kv, tp = lax.axis_index("kv"), lax.axis_index("tp")
    z, y = lax.div(kv, PAIR), lax.rem(kv, PAIR)
    n_x = n_tp // CORES
    cx, core = lax.div(tp, CORES), lax.rem(tp, CORES)
    batch, block = x_hbm.shape
    loads = {}

    def load(name, src, dst, sem):
        loads[name] = pltpu.make_async_copy(src, dst, sem)
        loads[name].start()

    load("x", x_hbm, pack.at[tp, pl.ds(0, batch)], in_sem.at[0])
    load("mg", mg_hbm, gain_in.at[0], in_sem.at[1])
    load("cg", cg_hbm, gain_in.at[1], in_sem.at[2])
    for i, (name, src, dst) in enumerate(
        [("q", qw_hbm, qw), ("k", kw_hbm, kw), ("v", vw_hbm, vw), ("g", gw_hbm, gw)]
    ):
        load(name, src, dst, w_sem.at[i])
    barrier = pltpu.get_barrier_semaphore()
    for d in range(1, n_kv):
        pl.semaphore_signal(
            barrier, inc=1, device_id={"kv": lax.rem(kv + d, n_kv)}, device_id_type=MESH
        )
    for d in range(1, n_tp):
        pl.semaphore_signal(
            barrier, inc=1, device_id={"tp": lax.rem(tp + d, n_tp)}, device_id_type=MESH
        )
    for name in ("x", "mg", "cg"):
        loads[name].wait()
    for i in range(2):
        gain = jnp.broadcast_to(gain_in[i].astype(F32), (GAIN_ROWS, block))
        pack[tp, batch + i * GAIN_ROWS : batch + (i + 1) * GAIN_ROWS] = gain.astype(BF16)
    pl.semaphore_wait(barrier, n_tp + n_kv - 2)
    x_copies = tp_gather(pack, tp, n_tp, t_sem)
    load("old", old_hbm, held, s_sem)
    for copy in x_copies:
        copy.wait_recv()

    def normalise(stream, row):
        parts = [
            (stream[t] * pack[t, row : row + GAIN_ROWS][:1].astype(F32)).astype(BF16)
            for t in range(n_tp)
        ]
        return jnp.concatenate(parts, axis=1)

    def squares_of(stream):
        return sum(jnp.sum(s * s, axis=1, keepdims=True) for s in stream)

    stream = [pack[t, :batch].astype(F32) for t in range(n_tp)]
    normed = normalise(stream, batch)
    sq_copies, sq_total = own_square_total(
        squares_of(stream), sq_src, sq_dst, kv, n_kv, rows, sq_sem
    )
    scatter = PairScatter(kv, n_kv, rows, part, got, summed, got2, sem_a, sem_b)
    mix_gather = PairGather(kv, n_kv, mixes, mz_sem, my_sem)

    def project(p):
        h, kind = divmod(p, 3)
        if h == 0:
            for name in (("q", "k"), ("v",), ("g",))[kind]:
                loads[name].wait()
        if kind == 0:
            cols = slice(h * dk, (h + 1) * dk)
            return jnp.concatenate(
                [
                    jnp.dot(normed, qw[:, cols], preferred_element_type=F32),
                    jnp.dot(normed, kw[:, cols], preferred_element_type=F32),
                ],
                axis=1,
            )
        w = (vw, gw)[kind - 1]
        return jnp.dot(normed, w[:, h * dv : (h + 1) * dv], preferred_element_type=F32)

    def retain(h, query, key, value, gate):
        columns = query.T
        step = min(dk, 64)
        for s in range(rows):
            total = jnp.zeros((8, dv), F32)
            for r in range(0, dk, step):
                term = columns[r : r + step, s : s + 1] * held[s, h, r : r + step]
                total = total + jnp.sum(term.reshape(step // 8, 8, dv), axis=0)
            ret[s : s + 1] = jnp.sum(total, axis=0, keepdims=True)
        out = rate_ref[h] * ret[...] + jnp.sum(query * key, axis=1, keepdims=True) * value
        out = out * lax.rsqrt(jnp.mean(out * out, axis=1, keepdims=True) + EPS)
        mixes[h, z, y] = (jax.nn.silu(gate) * out).astype(BF16)

    def attend(h):
        if h == 0:
            loads["ow"].wait()
        term = jnp.dot(
            mix_gather.finish(h), ow[h * dv : (h + 1) * dv], preferred_element_type=F32
        )
        acc[...] = term if h == 0 else acc[...] + term

    pieces = 3 * heads
    scale, values = None, {}
    for s in range(pieces + LAG_A + LAG_B):
        if s < pieces:
            scatter.start(s, project(s))
        if s == 0:
            load("ow", ow_hbm, ow, w_sem.at[4])
            load("up", up_hbm, up, w_sem.at[5])
            load("down", down_hbm, down, w_sem.at[6])
        p = s - LAG_A
        if 0 <= p < pieces:
            scatter.middle(p)
        p = p - LAG_B
        if 0 <= p < pieces:
            if p == 0:
                scale = lax.rsqrt(sq_total() / dim + EPS)
            h, kind = divmod(p, 3)
            total = scatter.finish(p) * scale
            if kind == 0:
                query, key = total[:, :dk], total[:, dk:] * dk ** (-0.5)
                k_ref[:, h * dk : (h + 1) * dk] = key
                values["q"], values["k"] = query, key
            elif kind == 1:
                v_ref[:, h * dv : (h + 1) * dv] = total
                values["v"] = total
            else:
                if h == 0:
                    loads["old"].wait()
                retain(h, values["q"], values["k"], values["v"], total)
                mix_gather.start(h)
                if h >= 1:
                    mix_gather.relay(h - 1)
                if h >= 2:
                    attend(h - 2)
    mix_gather.relay(heads - 1)
    for h in range(max(heads - 2, 0), heads):
        attend(h)

    half = pair_own.shape[1] // 2
    pair_own[...] = acc[...].astype(BF16)
    pair_copy = put(
        pair_own, pair_got, c_sem.at[0], c_sem.at[1], {"tp": cx * CORES + 1 - core}
    )
    pair_copy.wait_recv()
    both = pair_own[...].astype(F32) + pair_got[...].astype(F32)
    for j in range(CORES):
        chip[j] = both[:, j * half : (j + 1) * half].astype(BF16)
    far_copies = []
    for d in range(1, n_x):
        for rel in range(CORES):
            peer = lax.rem(cx + d, n_x) * CORES + lax.rem(core + rel, CORES)
            far_copies.append(
                put(
                    chip.at[core],
                    far.at[d - 1, rel],
                    far_sem.at[0, d - 1, rel],
                    far_sem.at[1, d - 1, rel],
                    {"tp": peer},
                )
            )
    for copy in far_copies:
        copy.wait_recv()
    sums = []
    for j in range(CORES):
        total = chip[j].astype(F32)
        for d in range(n_x - 1):
            total = total + far[d, lax.rem(core + j, CORES)].astype(F32)
        sums.append(total)
    attention = jnp.concatenate(sums, axis=1)
    for t in range(n_tp):
        mids[t] = (
            pack[t, :batch].astype(F32) + attention[:, t * block : (t + 1) * block]
        ).astype(BF16)
    stream = [mids[t].astype(F32) for t in range(n_tp)]
    normed_mid = normalise(stream, batch + GAIN_ROWS)
    sq_copies2, sq_total2 = own_square_total(
        squares_of(stream), sq_src2, sq_dst2, kv, n_kv, rows, sq_sem2
    )
    lift = PairScatter(kv, n_kv, rows, part_u, got_u, summed_u, got2_u, sem_ua, sem_ub)
    gather = PairGather(kv, n_kv, hid, hz_sem, hy_sem)
    count = up.shape[1] // width
    loads["up"].wait()
    scale2 = None
    for s in range(count + LAG_1 + LAG_2 + LAG_3 + LAG_4):
        if s < count:
            w = up[:, s * width : (s + 1) * width]
            lift.start(s, jnp.dot(normed_mid, w, preferred_element_type=F32))
        p = s - LAG_1
        if 0 <= p < count:
            lift.middle(p)
        p = p - LAG_2
        if 0 <= p < count:
            if p == 0:
                scale2 = lax.rsqrt(sq_total2() / dim + EPS)
            lifted = lift.finish(p) * scale2
            hid[p, z, y] = jnp.square(jnp.maximum(lifted, 0.0)).astype(BF16)
            gather.start(p)
        p = p - LAG_3
        if 0 <= p < count:
            gather.relay(p)
        p = p - LAG_4
        if 0 <= p < count:
            if p == 0:
                loads["down"].wait()
            w = down[p * width : (p + 1) * width]
            term = jnp.dot(gather.finish(p), w, preferred_element_type=F32)
            acc[...] = term if p == 0 else acc[...] + term
    for t in range(n_tp):
        ends[t] = acc[:, t * block : (t + 1) * block].astype(BF16)
    f_copies = tp_scatter(ends, got_ends, tp, n_tp, f_sem)
    lowered = ends[tp].astype(F32)
    for d, copy in enumerate(f_copies):
        copy.wait_recv()
        lowered = lowered + got_ends[d].astype(F32)
    out_ref[...] = (mids[tp].astype(F32) + lowered).astype(BF16)
    for group in (scatter, mix_gather, lift, gather):
        group.drain()
    rest = x_copies + sq_copies + sq_copies2 + far_copies + f_copies
    for copy in rest + [pair_copy]:
        copy.wait_send()


def state_kernel(heads, dk, dv, k_ref, v_ref, act_ref, rate_ref, old_ref, *refs):
    act_out, out_ref, new_ref, sem, act_sem = refs
    step = min(dk, 64)
    seqs = k_ref.shape[0]
    act_copy = pltpu.make_async_copy(act_ref, act_out, act_sem)
    act_copy.start()

    def write(s, h):
        return pltpu.make_async_copy(new_ref.at[s, h], out_ref.at[s, h], sem.at[s, h])

    def one(s, carry):
        k_row = k_ref[pl.ds(s, 1), :]
        lines = [k_row[:, h * dk : (h + 1) * dk] for h in range(heads)]
        lines.append(jnp.zeros((-heads % 8, dk), F32))
        columns = jnp.concatenate(lines, axis=0).T
        for h in range(heads):
            value = v_ref[pl.ds(s, 1), h * dv : (h + 1) * dv]
            for r in range(0, dk, step):
                key = columns[r : r + step, h : h + 1]
                new_ref[s, h, r : r + step] = (
                    rate_ref[h] * old_ref[s, h, r : r + step] + key * value
                )
            write(s, h).start()
        return carry

    lax.fori_loop(0, seqs, one, 0, unroll=2)
    for s in range(seqs):
        for h in range(heads):
            write(s, h).wait()
    act_copy.wait()


def in_hbm(a):
    return pltpu.with_memory_space_constraint(a, pltpu.HBM)


VM = pl.BlockSpec(memory_space=pltpu.VMEM)
SM = pl.BlockSpec(memory_space=pltpu.SMEM)
ANY = pl.BlockSpec(memory_space=pltpu.HBM)


def scatter_scratch(count, n_kv, rows, width):
    n_z = n_kv // PAIR
    return [
        pltpu.VMEM((count, PAIR, n_z, rows, width), BF16),
        pltpu.VMEM((count, n_z, rows, width), BF16),
        pltpu.VMEM((count, n_z, rows, width), BF16),
        pltpu.VMEM((count, n_z - 1, rows, width), BF16),
    ]


def fused_device(n_kv, n_tp, x, mg, cg, qw, kw, vw, gw, ow, uw, dw, state):
    seqs, heads, dk, dv = state.shape
    batch, block = x.shape
    dim = block * n_kv * n_tp
    n_z, n_x = n_kv // PAIR, n_tp // CORES
    depth, cols = qw.shape[0], ow.shape[1]
    width = min(WIDTH, uw.shape[1])
    count, pieces = uw.shape[1] // width, 3 * heads
    rates = lax.dynamic_slice_in_dim(
        head_decays(HEADS), lax.axis_index("tp") * heads, heads, 0
    )
    elements = sum(w.size for w in (qw, kw, vw, gw, ow, uw, dw))
    out, key, value, held = pl.pallas_call(
        functools.partial(fused_kernel, (n_kv, n_tp, seqs, width, dk, dv, heads, dim)),
        out_shape=[
            jax.ShapeDtypeStruct((batch, block), BF16),
            jax.ShapeDtypeStruct((seqs, heads * dk), F32),
            jax.ShapeDtypeStruct((seqs, heads * dv), F32),
            pltpu.VMEM(state.shape, F32),
        ],
        in_specs=[SM] + [ANY] * 11,
        out_specs=[VM] * 4,
        scratch_shapes=[
            pltpu.VMEM((n_tp, batch + 2 * GAIN_ROWS, block), BF16),
            pltpu.VMEM((2, 1, block), BF16),
            *[pltpu.VMEM(w.shape, BF16) for w in (qw, kw, vw, gw, ow, uw, dw)],
            *scatter_scratch(pieces, n_kv, seqs, dv),
            *scatter_scratch(count, n_kv, seqs, width),
            pltpu.VMEM((n_kv, seqs, 128), F32),
            pltpu.VMEM((n_kv - 1, seqs, 128), F32),
            pltpu.VMEM((n_kv, seqs, 128), F32),
            pltpu.VMEM((n_kv - 1, seqs, 128), F32),
            pltpu.VMEM((heads, n_z, PAIR, seqs, dv), BF16),
            pltpu.VMEM((count, n_z, PAIR, seqs, width), BF16),
            pltpu.VMEM((seqs, dv), F32),
            pltpu.VMEM((batch, cols), F32),
            pltpu.VMEM((batch, cols), BF16),
            pltpu.VMEM((batch, cols), BF16),
            pltpu.VMEM((CORES, batch, cols // CORES), BF16),
            pltpu.VMEM((max(n_x - 1, 1), CORES, batch, cols // CORES), BF16),
            pltpu.VMEM((n_tp, batch, block), BF16),
            pltpu.VMEM((n_tp, batch, block), BF16),
            pltpu.VMEM((n_tp - 1, batch, block), BF16),
            DMA((7,)),
            DMA,
            DMA((3,)),
            DMA((2, n_tp - 1)),
            DMA((2, n_kv - 1)),
            DMA((2, n_kv - 1)),
            DMA((2, pieces)),
            DMA((2, pieces, n_z - 1)),
            DMA((2, count)),
            DMA((2, count, n_z - 1)),
            DMA((2, heads, n_z - 1)),
            DMA((2, heads, n_z)),
            DMA((2, count, n_z - 1)),
            DMA((2, count, n_z)),
            DMA((2,)),
            DMA((2, max(n_x - 1, 1), CORES)),
            DMA((2, n_tp - 1)),
        ],
        compiler_params=pltpu.CompilerParams(
            collective_id=0, has_side_effects=True, vmem_limit_bytes=26 * 2**20
        ),
        cost_estimate=pl.CostEstimate(
            flops=2 * batch * elements,
            bytes_accessed=2 * elements + 4 * state.size,
            transcendentals=0,
        ),
        name="fused",
    )(
        rates,
        *[in_hbm(a) for a in (x, mg.reshape(1, block), cg.reshape(1, block))],
        *[in_hbm(a) for a in (qw, kw, vw, gw, ow, uw, dw, state)],
    )
    return pl.pallas_call(
        functools.partial(state_kernel, heads, dk, dv),
        out_shape=[pltpu.HBM((batch, block), BF16), pltpu.HBM(state.shape, F32)],
        in_specs=[VM, VM, VM, SM, VM],
        out_specs=[ANY, ANY],
        scratch_shapes=[pltpu.VMEM(state.shape, F32), DMA((seqs, heads)), DMA],
        compiler_params=pltpu.CompilerParams(vmem_limit_bytes=18 * 2**20),
        cost_estimate=pl.CostEstimate(
            flops=3 * state.size, bytes_accessed=8 * state.size, transcendentals=0
        ),
        name="state",
    )(key, value, out, rates, held)


def solution(mesh):
    return jax.shard_map(
        functools.partial(fused_device, mesh.shape["kv"], mesh.shape["tp"]),
        mesh=mesh,
        in_specs=(
            P(None, ("kv", "tp")),
            P(("kv", "tp")),
            P(("kv", "tp")),
            P("kv", "tp"),
            P("kv", "tp"),
            P("kv", "tp"),
            P("kv", "tp"),
            P("tp", "kv"),
            P("kv", "tp"),
            P("tp", "kv"),
            P("kv", "tp", None, None),
        ),
        out_specs=(P(None, ("kv", "tp")), P("kv", "tp", None, None)),
        check_vma=False,
    )
```

```python
import functools

import jax
import jax.numpy as jnp
from jax import lax
from jax.experimental import pallas as pl
from jax.experimental.pallas import tpu as pltpu
from jax.sharding import PartitionSpec as P

HEADS = 16
EPS = 1e-06
MESH = pl.DeviceIdType.MESH
F32 = jnp.float32
BF16 = jnp.bfloat16
DMA = pltpu.SemaphoreType.DMA
PAIR = 2
CORES = 2
GAIN_ROWS = 16
WIDTH = 512
LAG_A, LAG_B = 5, 5
LAG_1, LAG_2, LAG_3, LAG_4 = 4, 4, 4, 3


def head_decays(count):
    index = jnp.arange(count, dtype=jnp.float32)
    return 1.0 - 2.0 ** (-1.0 - 6.0 * index / (count - 1))


def put(src, dst, send_sem, recv_sem, where):
    copy = pltpu.make_async_remote_copy(
        src_ref=src,
        dst_ref=dst,
        send_sem=send_sem,
        recv_sem=recv_sem,
        device_id=where,
        device_id_type=MESH,
    )
    copy.start()
    return copy


def landed(ref, sem):
    pltpu.make_async_copy(ref, ref, sem).wait()


def tp_gather(buf, tp, n_tp, sems):
    for d in range(1, n_tp):
        put(buf.at[tp], buf.at[tp], sems.at[0], sems.at[1], {"tp": lax.rem(tp + d, n_tp)})


def tp_scatter(src, dst, tp, n_tp, sems):
    for d in range(1, n_tp):
        peer = lax.rem(tp + d, n_tp)
        put(src.at[peer], dst.at[d - 1], sems.at[0], sems.at[1], {"tp": peer})


def square_total(squares, sq_src, sq_dst, kv, n_kv, rows, sems):
    for g in range(n_kv):
        sq_src[g] = jnp.broadcast_to(squares[g * rows : (g + 1) * rows], sq_src.shape[1:])
    for d in range(1, n_kv):
        peer = lax.rem(kv + d, n_kv)
        put(sq_src.at[peer], sq_dst.at[d - 1], sems.at[0], sems.at[1], {"kv": peer})

    def finish():
        landed(sq_dst, sems.at[1])
        total = sq_src[kv]
        for d in range(n_kv - 1):
            total = total + sq_dst[d]
        return total[:, :1]

    return finish


class PairScatter:
    def __init__(self, kv, n_kv, rows, part, got, summed, got2, sends, sem_a, sem_b):
        self.n_z = n_kv // PAIR
        self.z, self.y = lax.div(kv, PAIR), lax.rem(kv, PAIR)
        self.rows = rows
        self.part, self.got, self.summed, self.got2 = part, got, summed, got2
        self.sends, self.sem_a, self.sem_b = sends, sem_a, sem_b

    def start(self, p, value):
        rows = self.rows
        for z in range(self.n_z):
            for y in range(PAIR):
                at = (z * PAIR + y) * rows
                self.part[p, y, z] = value[at : at + rows].astype(BF16)
        other = 1 - self.y
        put(
            self.part.at[p, other],
            self.got.at[p],
            self.sends.at[0],
            self.sem_a.at[p],
            {"kv": self.z * PAIR + other},
        )

    def middle(self, p):
        landed(self.got.at[p], self.sem_a.at[p])
        self.summed[p] = (self.part[p, self.y].astype(F32) + self.got[p].astype(F32)).astype(BF16)
        for d in range(1, self.n_z):
            peer = lax.rem(self.z + d, self.n_z)
            put(
                self.summed.at[p, peer],
                self.got2.at[p, d - 1],
                self.sends.at[1],
                self.sem_b.at[p],
                {"kv": peer * PAIR + self.y},
            )

    def finish(self, p):
        landed(self.got2.at[p], self.sem_b.at[p])
        total = self.summed[p, self.z].astype(F32)
        for d in range(self.n_z - 1):
            total = total + self.got2[p, d].astype(F32)
        return total

    def drain(self):
        landed(self.got, self.sends.at[0])
        landed(self.got2, self.sends.at[1])


class PairGather:
    def __init__(self, kv, n_kv, buf, sends, sem_z, sem_y):
        self.n_z = n_kv // PAIR
        self.z, self.y = lax.div(kv, PAIR), lax.rem(kv, PAIR)
        self.buf, self.sends, self.sem_z, self.sem_y = buf, sends, sem_z, sem_y

    def start(self, p):
        own = self.buf.at[p, self.z, self.y]
        for d in range(1, self.n_z):
            peer = lax.rem(self.z + d, self.n_z)
            put(own, own, self.sends.at[0], self.sem_z.at[p], {"kv": peer * PAIR + self.y})

    def relay(self, p):
        landed(self.buf.at[p, pl.ds(0, self.n_z - 1), 0], self.sem_z.at[p])
        put(
            self.buf.at[p, :, self.y],
            self.buf.at[p, :, self.y],
            self.sends.at[1],
            self.sem_y.at[p],
            {"kv": self.z * PAIR + 1 - self.y},
        )

    def finish(self, p):
        landed(self.buf.at[p, :, 0], self.sem_y.at[p])
        blocks = [
            self.buf[p, z, y].astype(F32) for z in range(self.n_z) for y in range(PAIR)
        ]
        return jnp.concatenate(blocks, axis=0).astype(BF16)

    def drain(self):
        landed(self.buf.at[:, pl.ds(0, self.n_z - 1), 0], self.sends.at[0])
        landed(self.buf.at[:, :, 0], self.sends.at[1])


def fused_kernel(sizes, rate_ref, x_hbm, mg_hbm, cg_hbm, *refs):
    n_kv, n_tp, rows, width, dk, dv, heads, dim = sizes
    (qw_hbm, kw_hbm, vw_hbm, gw_hbm, ow_hbm, up_hbm, down_hbm, old_hbm) = refs[:8]
    (out_ref, k_ref, v_ref, held) = refs[8:12]
    (pack, gain_in, qw, kw, vw, gw, ow, up, down) = refs[12:21]
    (part, got, summed, got2, part_u, got_u, summed_u, got2_u) = refs[21:29]
    (sq_src, sq_dst, sq_src2, sq_dst2, mixes, hid, ret, acc) = refs[29:37]
    (pair_own, pair_got, chip, far, mids, ends, got_ends) = refs[37:44]
    (w_sem, s_sem, in_sem, t_sem, sq_sem, sq_sem2) = refs[44:50]
    (sem_a, sem_b, sem_ua, sem_ub, mz_sem, my_sem, hz_sem, hy_sem) = refs[50:58]
    (c_sem, far_sem, f_sem, s_send, u_send, m_send, h_send) = refs[58:65]
    kv, tp = lax.axis_index("kv"), lax.axis_index("tp")
    z, y = lax.div(kv, PAIR), lax.rem(kv, PAIR)
    n_x = n_tp // CORES
    cx, core = lax.div(tp, CORES), lax.rem(tp, CORES)
    batch, block = x_hbm.shape
    loads = {}

    def load(name, src, dst, sem):
        loads[name] = pltpu.make_async_copy(src, dst, sem)
        loads[name].start()

    barrier = pltpu.get_barrier_semaphore()
    for d in range(1, n_kv):
        pl.semaphore_signal(
            barrier, inc=1, device_id={"kv": lax.rem(kv + d, n_kv)}, device_id_type=MESH
        )
    for d in range(1, n_tp):
        pl.semaphore_signal(
            barrier, inc=1, device_id={"tp": lax.rem(tp + d, n_tp)}, device_id_type=MESH
        )
    load("x", x_hbm, pack.at[tp, pl.ds(0, batch)], in_sem.at[0])
    load("mg", mg_hbm, gain_in.at[0], in_sem.at[1])
    load("cg", cg_hbm, gain_in.at[1], in_sem.at[2])
    for name in ("x", "mg", "cg"):
        loads[name].wait()
    for i, (name, src, dst) in enumerate(
        [("q", qw_hbm, qw), ("k", kw_hbm, kw), ("v", vw_hbm, vw), ("g", gw_hbm, gw)]
    ):
        load(name, src, dst, w_sem.at[i])
    for i in range(2):
        gain = jnp.broadcast_to(gain_in[i].astype(F32), (GAIN_ROWS, block))
        pack[tp, batch + i * GAIN_ROWS : batch + (i + 1) * GAIN_ROWS] = gain.astype(BF16)
    pl.semaphore_wait(barrier, n_tp + n_kv - 2)
    tp_gather(pack, tp, n_tp, t_sem)
    load("old", old_hbm, held, s_sem)
    landed(pack.at[pl.ds(0, n_tp - 1)], t_sem.at[1])

    def normalise(stream, row):
        parts = [
            (stream[t] * pack[t, row : row + GAIN_ROWS][:1].astype(F32)).astype(BF16)
            for t in range(n_tp)
        ]
        return jnp.concatenate(parts, axis=1)

    def squares_of(stream):
        return sum(jnp.sum(s * s, axis=1, keepdims=True) for s in stream)

    stream = [pack[t, :batch].astype(F32) for t in range(n_tp)]
    normed = normalise(stream, batch)
    sq_total = square_total(squares_of(stream), sq_src, sq_dst, kv, n_kv, rows, sq_sem)
    scatter = PairScatter(kv, n_kv, rows, part, got, summed, got2, s_send, sem_a, sem_b)
    mix_gather = PairGather(kv, n_kv, mixes, m_send, mz_sem, my_sem)

    def project(p):
        h, kind = divmod(p, 3)
        if h == 0:
            for name in (("q", "k"), ("v",), ("g",))[kind]:
                loads[name].wait()
        if kind == 0:
            cols = slice(h * dk, (h + 1) * dk)
            return jnp.concatenate(
                [
                    jnp.dot(normed, qw[:, cols], preferred_element_type=F32),
                    jnp.dot(normed, kw[:, cols], preferred_element_type=F32),
                ],
                axis=1,
            )
        w = (vw, gw)[kind - 1]
        return jnp.dot(normed, w[:, h * dv : (h + 1) * dv], preferred_element_type=F32)

    def retain(h, query, key, value, gate):
        columns = query.T
        step = min(dk, 64)
        for s in range(rows):
            total = jnp.zeros((8, dv), F32)
            for r in range(0, dk, step):
                term = columns[r : r + step, s : s + 1] * held[s, h, r : r + step]
                total = total + jnp.sum(term.reshape(step // 8, 8, dv), axis=0)
            ret[s : s + 1] = jnp.sum(total, axis=0, keepdims=True)
        out = rate_ref[h] * ret[...] + jnp.sum(query * key, axis=1, keepdims=True) * value
        out = out * lax.rsqrt(jnp.mean(out * out, axis=1, keepdims=True) + EPS)
        mixes[h, z, y] = (jax.nn.silu(gate) * out).astype(BF16)

    def attend(h):
        if h == 0:
            loads["ow"].wait()
        term = jnp.dot(
            mix_gather.finish(h), ow[h * dv : (h + 1) * dv], preferred_element_type=F32
        )
        acc[...] = term if h == 0 else acc[...] + term

    pieces = 3 * heads
    scale, values = None, {}
    for s in range(pieces + LAG_A + LAG_B):
        if s < pieces:
            scatter.start(s, project(s))
        if s == 0:
            load("ow", ow_hbm, ow, w_sem.at[4])
            load("up", up_hbm, up, w_sem.at[5])
            load("down", down_hbm, down, w_sem.at[6])
        p = s - LAG_A
        if 0 <= p < pieces:
            scatter.middle(p)
        p = p - LAG_B
        if 0 <= p < pieces:
            if p == 0:
                scale = lax.rsqrt(sq_total() / dim + EPS)
            h, kind = divmod(p, 3)
            total = scatter.finish(p) * scale
            if kind == 0:
                query, key = total[:, :dk], total[:, dk:] * dk ** (-0.5)
                k_ref[:, h * dk : (h + 1) * dk] = key
                values["q"], values["k"] = query, key
            elif kind == 1:
                v_ref[:, h * dv : (h + 1) * dv] = total
                values["v"] = total
            else:
                if h == 0:
                    loads["old"].wait()
                retain(h, values["q"], values["k"], values["v"], total)
                mix_gather.start(h)
                if h == heads - 1:
                    for g in range(max(heads - 1, 0)):
                        mix_gather.relay(g)
                    for g in range(max(heads - 2, 0)):
                        attend(g)
    mix_gather.relay(heads - 1)
    for h in range(max(heads - 2, 0), heads):
        attend(h)

    half = pair_own.shape[1] // 2
    pair_own[...] = acc[...].astype(BF16)
    pair_copy = put(
        pair_own, pair_got, c_sem.at[0], c_sem.at[1], {"tp": cx * CORES + 1 - core}
    )
    pair_copy.wait_recv()
    both = pair_own[...].astype(F32) + pair_got[...].astype(F32)
    for j in range(CORES):
        chip[j] = both[:, j * half : (j + 1) * half].astype(BF16)
    for d in range(1, n_x):
        for rel in range(CORES):
            peer = lax.rem(cx + d, n_x) * CORES + lax.rem(core + rel, CORES)
            put(
                chip.at[core],
                far.at[d - 1, rel],
                far_sem.at[0],
                far_sem.at[1],
                {"tp": peer},
            )
    landed(far, far_sem.at[1])
    sums = []
    for j in range(CORES):
        total = chip[j].astype(F32)
        for d in range(n_x - 1):
            total = total + far[d, lax.rem(core + j, CORES)].astype(F32)
        sums.append(total)
    attention = jnp.concatenate(sums, axis=1)
    for t in range(n_tp):
        mids[t] = (
            pack[t, :batch].astype(F32) + attention[:, t * block : (t + 1) * block]
        ).astype(BF16)
    stream = [mids[t].astype(F32) for t in range(n_tp)]
    normed_mid = normalise(stream, batch + GAIN_ROWS)
    sq_total2 = square_total(squares_of(stream), sq_src2, sq_dst2, kv, n_kv, rows, sq_sem2)
    lift = PairScatter(
        kv, n_kv, rows, part_u, got_u, summed_u, got2_u, u_send, sem_ua, sem_ub
    )
    gather = PairGather(kv, n_kv, hid, h_send, hz_sem, hy_sem)
    count = up.shape[1] // width
    loads["up"].wait()
    scale2 = None
    for s in range(count + LAG_1 + LAG_2 + LAG_3 + LAG_4):
        if s < count:
            w = up[:, s * width : (s + 1) * width]
            lift.start(s, jnp.dot(normed_mid, w, preferred_element_type=F32))
        p = s - LAG_1
        if 0 <= p < count:
            lift.middle(p)
        p = p - LAG_2
        if 0 <= p < count:
            if p == 0:
                scale2 = lax.rsqrt(sq_total2() / dim + EPS)
            lifted = lift.finish(p) * scale2
            hid[p, z, y] = jnp.square(jnp.maximum(lifted, 0.0)).astype(BF16)
            gather.start(p)
        p = p - LAG_3
        if 0 <= p < count:
            gather.relay(p)
        p = p - LAG_4
        if 0 <= p < count:
            if p == 0:
                loads["down"].wait()
            w = down[p * width : (p + 1) * width]
            term = jnp.dot(gather.finish(p), w, preferred_element_type=F32)
            acc[...] = term if p == 0 else acc[...] + term
    for t in range(n_tp):
        ends[t] = acc[:, t * block : (t + 1) * block].astype(BF16)
    tp_scatter(ends, got_ends, tp, n_tp, f_sem)
    landed(got_ends, f_sem.at[1])
    lowered = ends[tp].astype(F32)
    for d in range(n_tp - 1):
        lowered = lowered + got_ends[d].astype(F32)
    out_ref[...] = (mids[tp].astype(F32) + lowered).astype(BF16)
    for group in (scatter, mix_gather, lift, gather):
        group.drain()
    pair_copy.wait_send()
    landed(pack.at[pl.ds(0, n_tp - 1)], t_sem.at[0])
    landed(sq_dst, sq_sem.at[0])
    landed(sq_dst2, sq_sem2.at[0])
    landed(far, far_sem.at[0])
    landed(got_ends, f_sem.at[0])


def state_kernel(heads, dk, dv, k_ref, v_ref, act_ref, rate_ref, old_ref, *refs):
    act_out, out_ref, new_ref, sem, act_sem = refs
    step = min(dk, 64)
    seqs = k_ref.shape[0]
    act_copy = pltpu.make_async_copy(act_ref, act_out, act_sem)
    act_copy.start()

    def write(s, h):
        return pltpu.make_async_copy(new_ref.at[s, h], out_ref.at[s, h], sem.at[s, h])

    def one(s, carry):
        k_row = k_ref[pl.ds(s, 1), :]
        lines = [k_row[:, h * dk : (h + 1) * dk] for h in range(heads)]
        lines.append(jnp.zeros((-heads % 8, dk), F32))
        columns = jnp.concatenate(lines, axis=0).T
        for h in range(heads):
            value = v_ref[pl.ds(s, 1), h * dv : (h + 1) * dv]
            for r in range(0, dk, step):
                key = columns[r : r + step, h : h + 1]
                new_ref[s, h, r : r + step] = (
                    rate_ref[h] * old_ref[s, h, r : r + step] + key * value
                )
            write(s, h).start()
        return carry

    lax.fori_loop(0, seqs, one, 0, unroll=2)
    for s in range(seqs):
        for h in range(heads):
            write(s, h).wait()
    act_copy.wait()


def in_hbm(a):
    return pltpu.with_memory_space_constraint(a, pltpu.HBM)


VM = pl.BlockSpec(memory_space=pltpu.VMEM)
SM = pl.BlockSpec(memory_space=pltpu.SMEM)
ANY = pl.BlockSpec(memory_space=pltpu.HBM)


def scatter_scratch(count, n_kv, rows, width):
    n_z = n_kv // PAIR
    return [
        pltpu.VMEM((count, PAIR, n_z, rows, width), BF16),
        pltpu.VMEM((count, n_z, rows, width), BF16),
        pltpu.VMEM((count, n_z, rows, width), BF16),
        pltpu.VMEM((count, n_z - 1, rows, width), BF16),
    ]


def fused_device(n_kv, n_tp, x, mg, cg, qw, kw, vw, gw, ow, uw, dw, state):
    seqs, heads, dk, dv = state.shape
    batch, block = x.shape
    dim = block * n_kv * n_tp
    n_z, n_x = n_kv // PAIR, n_tp // CORES
    depth, cols = qw.shape[0], ow.shape[1]
    width = min(WIDTH, uw.shape[1])
    count, pieces = uw.shape[1] // width, 3 * heads
    rates = lax.dynamic_slice_in_dim(
        head_decays(HEADS), lax.axis_index("tp") * heads, heads, 0
    )
    elements = sum(w.size for w in (qw, kw, vw, gw, ow, uw, dw))
    out, key, value, held = pl.pallas_call(
        functools.partial(fused_kernel, (n_kv, n_tp, seqs, width, dk, dv, heads, dim)),
        out_shape=[
            jax.ShapeDtypeStruct((batch, block), BF16),
            jax.ShapeDtypeStruct((seqs, heads * dk), F32),
            jax.ShapeDtypeStruct((seqs, heads * dv), F32),
            pltpu.VMEM(state.shape, F32),
        ],
        in_specs=[SM] + [ANY] * 11,
        out_specs=[VM] * 4,
        scratch_shapes=[
            pltpu.VMEM((n_tp, batch + 2 * GAIN_ROWS, block), BF16),
            pltpu.VMEM((2, 1, block), BF16),
            *[pltpu.VMEM(w.shape, BF16) for w in (qw, kw, vw, gw, ow, uw, dw)],
            *scatter_scratch(pieces, n_kv, seqs, dv),
            *scatter_scratch(count, n_kv, seqs, width),
            pltpu.VMEM((n_kv, seqs, 128), F32),
            pltpu.VMEM((n_kv - 1, seqs, 128), F32),
            pltpu.VMEM((n_kv, seqs, 128), F32),
            pltpu.VMEM((n_kv - 1, seqs, 128), F32),
            pltpu.VMEM((heads, n_z, PAIR, seqs, dv), BF16),
            pltpu.VMEM((count, n_z, PAIR, seqs, width), BF16),
            pltpu.VMEM((seqs, dv), F32),
            pltpu.VMEM((batch, cols), F32),
            pltpu.VMEM((batch, cols), BF16),
            pltpu.VMEM((batch, cols), BF16),
            pltpu.VMEM((CORES, batch, cols // CORES), BF16),
            pltpu.VMEM((max(n_x - 1, 1), CORES, batch, cols // CORES), BF16),
            pltpu.VMEM((n_tp, batch, block), BF16),
            pltpu.VMEM((n_tp, batch, block), BF16),
            pltpu.VMEM((n_tp - 1, batch, block), BF16),
            DMA((7,)),
            DMA,
            DMA((3,)),
            *[DMA((2,))] * 3,
            *[DMA((pieces,))] * 2,
            *[DMA((count,))] * 2,
            *[DMA((heads,))] * 2,
            *[DMA((count,))] * 2,
            *[DMA((2,))] * 7,
        ],
        compiler_params=pltpu.CompilerParams(
            collective_id=0, has_side_effects=True, vmem_limit_bytes=26 * 2**20
        ),
        cost_estimate=pl.CostEstimate(
            flops=2 * batch * elements,
            bytes_accessed=2 * elements + 4 * state.size,
            transcendentals=0,
        ),
        name="fused",
    )(
        rates,
        *[in_hbm(a) for a in (x, mg.reshape(1, block), cg.reshape(1, block))],
        *[in_hbm(a) for a in (qw, kw, vw, gw, ow, uw, dw, state)],
    )
    return pl.pallas_call(
        functools.partial(state_kernel, heads, dk, dv),
        out_shape=[pltpu.HBM((batch, block), BF16), pltpu.HBM(state.shape, F32)],
        in_specs=[VM, VM, VM, SM, VM],
        out_specs=[ANY, ANY],
        scratch_shapes=[pltpu.VMEM(state.shape, F32), DMA((seqs, heads)), DMA],
        compiler_params=pltpu.CompilerParams(vmem_limit_bytes=18 * 2**20),
        cost_estimate=pl.CostEstimate(
            flops=3 * state.size, bytes_accessed=8 * state.size, transcendentals=0
        ),
        name="state",
    )(key, value, out, rates, held)


def solution(mesh):
    return jax.shard_map(
        functools.partial(fused_device, mesh.shape["kv"], mesh.shape["tp"]),
        mesh=mesh,
        in_specs=(
            P(None, ("kv", "tp")),
            P(("kv", "tp")),
            P(("kv", "tp")),
            P("kv", "tp"),
            P("kv", "tp"),
            P("kv", "tp"),
            P("kv", "tp"),
            P("tp", "kv"),
            P("kv", "tp"),
            P("tp", "kv"),
            P("kv", "tp", None, None),
        ),
        out_specs=(P(None, ("kv", "tp")), P("kv", "tp", None, None)),
        check_vma=False,
    )
```

```python
import functools

import jax
import jax.numpy as jnp
from jax import lax
from jax.experimental import pallas as pl
from jax.experimental.pallas import tpu as pltpu
from jax.sharding import PartitionSpec as P

HEADS = 16
EPS = 1e-06
MESH = pl.DeviceIdType.MESH
F32 = jnp.float32
BF16 = jnp.bfloat16
DMA = pltpu.SemaphoreType.DMA
PAIR = 2
CORES = 2
GAIN_ROWS = 16
WIDTH = 512
LAG_A, LAG_B = 5, 5
LAG_1, LAG_2, LAG_3, LAG_4 = 4, 4, 4, 3
DIRECT_A, DIRECT_M, DIRECT_U, DIRECT_H = 3, 2, 3, 2
HOLD, EARLY = 6, 2
FIRST = 0
CHUNKS = 1


def head_decays(count):
    index = jnp.arange(count, dtype=jnp.float32)
    return 1.0 - 2.0 ** (-1.0 - 6.0 * index / (count - 1))


def put(src, dst, send_sem, recv_sem, where):
    copy = pltpu.make_async_remote_copy(
        src_ref=src,
        dst_ref=dst,
        send_sem=send_sem,
        recv_sem=recv_sem,
        device_id=where,
        device_id_type=MESH,
    )
    copy.start()
    return copy


def landed(ref, sem):
    pltpu.make_async_copy(ref, ref, sem).wait()


def tp_gather(buf, tp, n_tp, sems):
    for d in range(1, n_tp):
        put(buf.at[tp], buf.at[tp], sems.at[0], sems.at[1], {"tp": lax.rem(tp + d, n_tp)})


def tp_scatter(src, dst, tp, n_tp, sems):
    for d in range(1, n_tp):
        peer = lax.rem(tp + d, n_tp)
        put(src.at[peer], dst.at[d - 1], sems.at[0], sems.at[1], {"tp": peer})


def square_total(squares, sq_src, sq_dst, kv, n_kv, rows, sems):
    for g in range(n_kv):
        sq_src[g] = jnp.broadcast_to(squares[g * rows : (g + 1) * rows], sq_src.shape[1:])
    for d in range(1, n_kv):
        peer = lax.rem(kv + d, n_kv)
        put(sq_src.at[peer], sq_dst.at[d - 1], sems.at[0], sems.at[1], {"kv": peer})

    def finish():
        landed(sq_dst, sems.at[1])
        total = sq_src[kv]
        for d in range(n_kv - 1):
            total = total + sq_dst[d]
        return total[:, :1]

    return finish


def send_order(s, direct):
    if s < FIRST:
        return s + direct
    return s - FIRST if s < FIRST + direct else s


class PairScatter:
    def __init__(self, kv, n_kv, rows, direct, bufs, sends, sem_a, sem_b):
        self.kv, self.n_kv, self.n_z = kv, n_kv, n_kv // PAIR
        self.z, self.y = lax.div(kv, PAIR), lax.rem(kv, PAIR)
        self.rows, self.direct = rows, direct
        self.part, self.got, self.summed, self.got2, self.got_all = bufs
        self.sends, self.sem_a, self.sem_b = sends, sem_a, sem_b

    def start(self, p, value):
        rows = self.rows
        for z in range(self.n_z):
            for y in range(PAIR):
                at = (z * PAIR + y) * rows
                self.part[p, y, z] = value[at : at + rows].astype(BF16)
        if p < self.direct:
            for d in range(1, self.n_kv):
                peer = lax.rem(self.kv + d, self.n_kv)
                put(
                    self.part.at[p, lax.rem(peer, PAIR), lax.div(peer, PAIR)],
                    self.got_all.at[p, d - 1],
                    self.sends.at[2],
                    self.sem_b.at[p],
                    {"kv": peer},
                )
            return
        other = 1 - self.y
        put(
            self.part.at[p, other],
            self.got.at[p],
            self.sends.at[0],
            self.sem_a.at[p],
            {"kv": self.z * PAIR + other},
        )

    def middle(self, p):
        if p < self.direct:
            return
        landed(self.got.at[p], self.sem_a.at[p])
        self.summed[p] = (self.part[p, self.y].astype(F32) + self.got[p].astype(F32)).astype(BF16)
        for d in range(1, self.n_z):
            peer = lax.rem(self.z + d, self.n_z)
            put(
                self.summed.at[p, peer],
                self.got2.at[p, d - 1],
                self.sends.at[1],
                self.sem_b.at[p],
                {"kv": peer * PAIR + self.y},
            )

    def finish(self, p):
        if p < self.direct:
            landed(self.got_all.at[p], self.sem_b.at[p])
            own, got = self.part[p, self.y, self.z], self.got_all
        else:
            landed(self.got2.at[p], self.sem_b.at[p])
            own, got = self.summed[p, self.z], self.got2
        total = own.astype(F32)
        for d in range(got.shape[1]):
            total = total + got[p, d].astype(F32)
        return total

    def drain(self):
        rest = pl.ds(self.direct, self.got.shape[0] - self.direct)
        landed(self.got.at[rest], self.sends.at[0])
        landed(self.got2.at[rest], self.sends.at[1])
        if self.direct:
            landed(self.got_all.at[pl.ds(0, self.direct)], self.sends.at[2])


class PairGather:
    def __init__(self, kv, n_kv, direct, buf, like, sends, sem_z, sem_y):
        self.kv, self.n_kv, self.n_z = kv, n_kv, n_kv // PAIR
        self.z, self.y = lax.div(kv, PAIR), lax.rem(kv, PAIR)
        self.relayed, self.direct = buf.shape[0] - direct, direct
        self.buf, self.like = buf, like
        self.sends, self.sem_z, self.sem_y = sends, sem_z, sem_y

    def start(self, p):
        own = self.buf.at[p, self.z, self.y]
        if p >= self.relayed:
            for d in range(1, self.n_kv):
                peer = {"kv": lax.rem(self.kv + d, self.n_kv)}
                put(own, own, self.sends.at[2], self.sem_z.at[p], peer)
            return
        for d in range(1, self.n_z):
            peer = lax.rem(self.z + d, self.n_z)
            put(own, own, self.sends.at[0], self.sem_z.at[p], {"kv": peer * PAIR + self.y})

    def relay(self, p):
        if p >= self.relayed:
            return
        landed(self.buf.at[p, pl.ds(0, self.n_z - 1), 0], self.sem_z.at[p])
        put(
            self.buf.at[p, :, self.y],
            self.buf.at[p, :, self.y],
            self.sends.at[1],
            self.sem_y.at[p],
            {"kv": self.z * PAIR + 1 - self.y},
        )

    def finish(self, p):
        if p >= self.relayed:
            landed(self.like.at[0], self.sem_z.at[p])
        else:
            landed(self.buf.at[p, :, 0], self.sem_y.at[p])
        blocks = [
            self.buf[p, z, y].astype(F32) for z in range(self.n_z) for y in range(PAIR)
        ]
        return jnp.concatenate(blocks, axis=0).astype(BF16)

    def drain(self):
        rest = pl.ds(0, self.relayed)
        landed(self.buf.at[rest, pl.ds(0, self.n_z - 1), 0], self.sends.at[0])
        landed(self.buf.at[rest, :, 0], self.sends.at[1])
        if self.direct:
            landed(self.like.at[pl.ds(0, self.direct)], self.sends.at[2])


def fused_kernel(sizes, rate_ref, x_hbm, mg_hbm, cg_hbm, *refs):
    n_kv, n_tp, rows, width, dk, dv, heads, dim = sizes
    (qw_hbm, kw_hbm, vw_hbm, gw_hbm, ow_hbm, up_hbm, down_hbm, old_hbm) = refs[:8]
    (out_ref, held) = refs[8:10]
    (pack, gain_in, qw, kw, vw, gw, ow, up, down) = refs[10:19]
    bufs, bufs_u, refs = refs[19:24], refs[24:29], refs[29:]
    (sq_src, sq_dst, sq_src2, sq_dst2, mixes, hid, ret, acc, keys, vals) = refs[:10]
    (pair_own, pair_got, chip, far, mids, ends, got_ends) = refs[10:17]
    (w_sem, s_sem, in_sem, t_sem, sq_sem, sq_sem2) = refs[17:23]
    (sems, sems_u, sems_m, sems_h) = refs[23:26], refs[26:29], refs[29:32], refs[32:35]
    (c_sem, far_sem, f_sem) = refs[35:38]
    kv, tp = lax.axis_index("kv"), lax.axis_index("tp")
    z, y = lax.div(kv, PAIR), lax.rem(kv, PAIR)
    n_x = n_tp // CORES
    cx, core = lax.div(tp, CORES), lax.rem(tp, CORES)
    batch, block = x_hbm.shape
    loads = {}

    def load(name, src, dst, sem):
        loads[name] = pltpu.make_async_copy(src, dst, sem)
        loads[name].start()

    barrier = pltpu.get_barrier_semaphore()
    for d in range(1, n_kv):
        pl.semaphore_signal(
            barrier, inc=1, device_id={"kv": lax.rem(kv + d, n_kv)}, device_id_type=MESH
        )
    for d in range(1, n_tp):
        pl.semaphore_signal(
            barrier, inc=1, device_id={"tp": lax.rem(tp + d, n_tp)}, device_id_type=MESH
        )
    load("x", x_hbm, pack.at[tp, pl.ds(0, batch)], in_sem.at[0])
    load("mg", mg_hbm, gain_in.at[0], in_sem.at[1])
    load("cg", cg_hbm, gain_in.at[1], in_sem.at[2])
    for name in ("x", "mg", "cg"):
        loads[name].wait()
    for i, (name, src, dst) in enumerate(
        [("q", qw_hbm, qw), ("k", kw_hbm, kw), ("v", vw_hbm, vw), ("g", gw_hbm, gw)]
    ):
        load(name, src, dst, w_sem.at[i])
    for i in range(2):
        gain = jnp.broadcast_to(gain_in[i].astype(F32), (GAIN_ROWS, block))
        pack[tp, batch + i * GAIN_ROWS : batch + (i + 1) * GAIN_ROWS] = gain.astype(BF16)
    pl.semaphore_wait(barrier, n_tp + n_kv - 2)
    tp_gather(pack, tp, n_tp, t_sem)
    load("old", old_hbm, held, s_sem)
    landed(pack.at[pl.ds(0, n_tp - 1)], t_sem.at[1])

    def normalise(stream, row):
        parts = [
            (stream[t] * pack[t, row : row + GAIN_ROWS][:1].astype(F32)).astype(BF16)
            for t in range(n_tp)
        ]
        return jnp.concatenate(parts, axis=1)

    def squares_of(stream):
        return sum(jnp.sum(s * s, axis=1, keepdims=True) for s in stream)

    stream = [pack[t, :batch].astype(F32) for t in range(n_tp)]
    normed = normalise(stream, batch)
    sq_total = square_total(squares_of(stream), sq_src, sq_dst, kv, n_kv, rows, sq_sem)
    scatter = PairScatter(kv, n_kv, rows, DIRECT_A, bufs, *sems)
    mix_gather = PairGather(kv, n_kv, DIRECT_M, mixes, bufs[4], *sems_m)

    ready = set()

    def project(p):
        h, kind = divmod(p, 3)
        for name in (("q", "k"), ("v",), ("g",))[kind]:
            if name not in ready:
                loads[name].wait()
                ready.add(name)
        if kind == 0:
            cols = slice(h * dk, (h + 1) * dk)
            return jnp.concatenate(
                [
                    jnp.dot(normed, qw[:, cols], preferred_element_type=F32),
                    jnp.dot(normed, kw[:, cols], preferred_element_type=F32),
                ],
                axis=1,
            )
        w = (vw, gw)[kind - 1]
        return jnp.dot(normed, w[:, h * dv : (h + 1) * dv], preferred_element_type=F32)

    def retain(h, query, key, value, gate):
        columns = query.T
        step = min(dk, 64)
        for s in range(rows):
            total = jnp.zeros((8, dv), F32)
            for r in range(0, dk, step):
                term = columns[r : r + step, s : s + 1] * held[s, h, r : r + step]
                total = total + jnp.sum(term.reshape(step // 8, 8, dv), axis=0)
            ret[s : s + 1] = jnp.sum(total, axis=0, keepdims=True)
        out = rate_ref[h] * ret[...] + jnp.sum(query * key, axis=1, keepdims=True) * value
        out = out * lax.rsqrt(jnp.mean(out * out, axis=1, keepdims=True) + EPS)
        mixes[h, z, y] = (jax.nn.silu(gate) * out).astype(BF16)

    def update(h):
        columns, value = keys[h].T, vals[h]
        step = min(dk, 64)
        for s in range(rows):
            line = value[s : s + 1]
            for r in range(0, dk, step):
                term = columns[r : r + step, s : s + 1] * line
                held[s, h, r : r + step] = rate_ref[h] * held[s, h, r : r + step] + term

    def attend(h):
        if h == 0:
            loads["ow"].wait()
        term = jnp.dot(
            mix_gather.finish(h), ow[h * dv : (h + 1) * dv], preferred_element_type=F32
        )
        acc[...] = term if h == 0 else acc[...] + term

    pieces = 3 * heads
    scale, values, pending = None, {}, []
    for s in range(pieces + LAG_A + LAG_B):
        if s < pieces:
            first = send_order(s, DIRECT_A)
            scatter.start(first, project(first))
        if s == 0:
            load("ow", ow_hbm, ow, w_sem.at[4])
            load("up", up_hbm, up, w_sem.at[5])
            load("down", down_hbm, down, w_sem.at[6])
        p = s - LAG_A
        if 0 <= p < pieces:
            scatter.middle(p)
        p = p - LAG_B
        if 0 <= p < pieces:
            if p == 0:
                scale = lax.rsqrt(sq_total() / dim + EPS)
            h, kind = divmod(p, 3)
            total = scatter.finish(p) * scale
            if kind == 0:
                query, key = total[:, :dk], total[:, dk:] * dk ** (-0.5)
                keys[h] = key
                values["q"], values["k"] = query, key
            elif kind == 1:
                vals[h] = total
                values["v"] = total
            else:
                if h == 0:
                    loads["old"].wait()
                retain(h, values["q"], values["k"], values["v"], total)
                if h < heads - 1:
                    pending.append(h)
                else:
                    mix_gather.start(h)
            if p >= HOLD:
                for g in pending:
                    mix_gather.start(g)
                pending = []
    for h in range(heads - 1):
        mix_gather.relay(h)
    for h in range(min(EARLY, heads - 1)):
        update(h)
    for h in range(heads):
        attend(h)

    half = pair_own.shape[1] // 2
    pair_own[...] = acc[...].astype(BF16)
    pair_copy = put(
        pair_own, pair_got, c_sem.at[0], c_sem.at[1], {"tp": cx * CORES + 1 - core}
    )
    pair_copy.wait_recv()
    both = pair_own[...].astype(F32) + pair_got[...].astype(F32)
    for j in range(CORES):
        chip[j] = both[:, j * half : (j + 1) * half].astype(BF16)
    for d in range(1, n_x):
        for rel in range(CORES):
            peer = lax.rem(cx + d, n_x) * CORES + lax.rem(core + rel, CORES)
            put(
                chip.at[core],
                far.at[d - 1, rel],
                far_sem.at[0],
                far_sem.at[1],
                {"tp": peer},
            )
    for h in range(min(EARLY, heads - 1), heads):
        update(h)
    landed(far, far_sem.at[1])
    sums = []
    for j in range(CORES):
        total = chip[j].astype(F32)
        for d in range(n_x - 1):
            total = total + far[d, lax.rem(core + j, CORES)].astype(F32)
        sums.append(total)
    attention = jnp.concatenate(sums, axis=1)
    for t in range(n_tp):
        mids[t] = (
            pack[t, :batch].astype(F32) + attention[:, t * block : (t + 1) * block]
        ).astype(BF16)
    stream = [mids[t].astype(F32) for t in range(n_tp)]
    normed_mid = normalise(stream, batch + GAIN_ROWS)
    sq_total2 = square_total(squares_of(stream), sq_src2, sq_dst2, kv, n_kv, rows, sq_sem2)
    lift = PairScatter(kv, n_kv, rows, DIRECT_U, bufs_u, *sems_u)
    gather = PairGather(kv, n_kv, DIRECT_H, hid, bufs_u[4], *sems_h)
    count = up.shape[1] // width
    loads["up"].wait()
    scale2 = None
    for s in range(count + LAG_1 + LAG_2 + LAG_3 + LAG_4):
        if s < count:
            first = send_order(s, DIRECT_U)
            w = up[:, first * width : (first + 1) * width]
            lift.start(first, jnp.dot(normed_mid, w, preferred_element_type=F32))
        p = s - LAG_1
        if 0 <= p < count:
            lift.middle(p)
        p = p - LAG_2
        if 0 <= p < count:
            if p == 0:
                scale2 = lax.rsqrt(sq_total2() / dim + EPS)
            lifted = lift.finish(p) * scale2
            hid[p, z, y] = jnp.square(jnp.maximum(lifted, 0.0)).astype(BF16)
            gather.start(p)
        p = p - LAG_3
        if 0 <= p < count:
            gather.relay(p)
        p = p - LAG_4
        if 0 <= p < count:
            if p == 0:
                loads["down"].wait()
            w = down[p * width : (p + 1) * width]
            term = jnp.dot(gather.finish(p), w, preferred_element_type=F32)
            acc[...] = term if p == 0 else acc[...] + term
    for t in range(n_tp):
        ends[t] = acc[:, t * block : (t + 1) * block].astype(BF16)
    tp_scatter(ends, got_ends, tp, n_tp, f_sem)
    landed(got_ends, f_sem.at[1])
    lowered = ends[tp].astype(F32)
    for d in range(n_tp - 1):
        lowered = lowered + got_ends[d].astype(F32)
    out_ref[...] = (mids[tp].astype(F32) + lowered).astype(BF16)
    for group in (scatter, mix_gather, lift, gather):
        group.drain()
    pair_copy.wait_send()
    landed(pack.at[pl.ds(0, n_tp - 1)], t_sem.at[0])
    landed(sq_dst, sq_sem.at[0])
    landed(sq_dst2, sq_sem2.at[0])
    landed(far, far_sem.at[0])
    landed(got_ends, f_sem.at[0])


def write_kernel(act_ref, state_ref, act_out, state_out, act_sem, sem):
    copies = [pltpu.make_async_copy(act_ref, act_out, act_sem)]
    for s in range(state_ref.shape[0]):
        for h in range(CHUNKS):
            n = state_ref.shape[1] // CHUNKS
            part = (s, pl.ds(h * n, n))
            copies.append(
                pltpu.make_async_copy(state_ref.at[part], state_out.at[part], sem.at[s, h])
            )
    for copy in copies:
        copy.start()
    for copy in copies:
        copy.wait()


def in_hbm(a):
    return pltpu.with_memory_space_constraint(a, pltpu.HBM)


VM = pl.BlockSpec(memory_space=pltpu.VMEM)
SM = pl.BlockSpec(memory_space=pltpu.SMEM)
ANY = pl.BlockSpec(memory_space=pltpu.HBM)


def scatter_scratch(count, n_kv, rows, width, direct):
    n_z = n_kv // PAIR
    return [
        pltpu.VMEM((count, PAIR, n_z, rows, width), BF16),
        pltpu.VMEM((count, n_z, rows, width), BF16),
        pltpu.VMEM((count, n_z, rows, width), BF16),
        pltpu.VMEM((count, n_z - 1, rows, width), BF16),
        pltpu.VMEM((max(direct, 1), n_kv - 1, rows, width), BF16),
    ]


def fused_device(n_kv, n_tp, x, mg, cg, qw, kw, vw, gw, ow, uw, dw, state):
    seqs, heads, dk, dv = state.shape
    batch, block = x.shape
    dim = block * n_kv * n_tp
    n_z, n_x = n_kv // PAIR, n_tp // CORES
    depth, cols = qw.shape[0], ow.shape[1]
    width = min(WIDTH, uw.shape[1])
    count, pieces = uw.shape[1] // width, 3 * heads
    rates = lax.dynamic_slice_in_dim(
        head_decays(HEADS), lax.axis_index("tp") * heads, heads, 0
    )
    elements = sum(w.size for w in (qw, kw, vw, gw, ow, uw, dw))
    out, held = pl.pallas_call(
        functools.partial(fused_kernel, (n_kv, n_tp, seqs, width, dk, dv, heads, dim)),
        out_shape=[
            jax.ShapeDtypeStruct((batch, block), BF16),
            pltpu.VMEM(state.shape, F32),
        ],
        in_specs=[SM] + [ANY] * 11,
        out_specs=[VM] * 2,
        scratch_shapes=[
            pltpu.VMEM((n_tp, batch + 2 * GAIN_ROWS, block), BF16),
            pltpu.VMEM((2, 1, block), BF16),
            *[pltpu.VMEM(w.shape, BF16) for w in (qw, kw, vw, gw, ow, uw, dw)],
            *scatter_scratch(pieces, n_kv, seqs, dv, max(DIRECT_A, DIRECT_M)),
            *scatter_scratch(count, n_kv, seqs, width, max(DIRECT_U, DIRECT_H)),
            pltpu.VMEM((n_kv, seqs, 128), F32),
            pltpu.VMEM((n_kv - 1, seqs, 128), F32),
            pltpu.VMEM((n_kv, seqs, 128), F32),
            pltpu.VMEM((n_kv - 1, seqs, 128), F32),
            pltpu.VMEM((heads, n_z, PAIR, seqs, dv), BF16),
            pltpu.VMEM((count, n_z, PAIR, seqs, width), BF16),
            pltpu.VMEM((seqs, dv), F32),
            pltpu.VMEM((batch, cols), F32),
            pltpu.VMEM((heads, seqs, dk), F32),
            pltpu.VMEM((heads, seqs, dv), F32),
            pltpu.VMEM((batch, cols), BF16),
            pltpu.VMEM((batch, cols), BF16),
            pltpu.VMEM((CORES, batch, cols // CORES), BF16),
            pltpu.VMEM((max(n_x - 1, 1), CORES, batch, cols // CORES), BF16),
            pltpu.VMEM((n_tp, batch, block), BF16),
            pltpu.VMEM((n_tp, batch, block), BF16),
            pltpu.VMEM((n_tp - 1, batch, block), BF16),
            DMA((7,)),
            DMA,
            DMA((3,)),
            *[DMA((2,))] * 3,
            *[DMA((3,)), *[DMA((pieces,))] * 2],
            *[DMA((3,)), *[DMA((count,))] * 2],
            *[DMA((3,)), *[DMA((heads,))] * 2],
            *[DMA((3,)), *[DMA((count,))] * 2],
            *[DMA((2,))] * 3,
        ],
        compiler_params=pltpu.CompilerParams(
            collective_id=0, has_side_effects=True, vmem_limit_bytes=26 * 2**20
        ),
        cost_estimate=pl.CostEstimate(
            flops=2 * batch * elements,
            bytes_accessed=2 * elements + 4 * state.size,
            transcendentals=0,
        ),
        name="fused",
    )(
        rates,
        *[in_hbm(a) for a in (x, mg.reshape(1, block), cg.reshape(1, block))],
        *[in_hbm(a) for a in (qw, kw, vw, gw, ow, uw, dw, state)],
    )
    return pl.pallas_call(
        write_kernel,
        out_shape=[pltpu.HBM((batch, block), BF16), pltpu.HBM(state.shape, F32)],
        in_specs=[VM, VM],
        out_specs=[ANY, ANY],
        scratch_shapes=[DMA, DMA((seqs, CHUNKS))],
        compiler_params=pltpu.CompilerParams(vmem_limit_bytes=2**20),
        cost_estimate=pl.CostEstimate(
            flops=state.size, bytes_accessed=4 * state.size, transcendentals=0
        ),
        name="write",
    )(out, held)


def solution(mesh):
    return jax.shard_map(
        functools.partial(fused_device, mesh.shape["kv"], mesh.shape["tp"]),
        mesh=mesh,
        in_specs=(
            P(None, ("kv", "tp")),
            P(("kv", "tp")),
            P(("kv", "tp")),
            P("kv", "tp"),
            P("kv", "tp"),
            P("kv", "tp"),
            P("kv", "tp"),
            P("tp", "kv"),
            P("kv", "tp"),
            P("tp", "kv"),
            P("kv", "tp", None, None),
        ),
        out_specs=(P(None, ("kv", "tp")), P("kv", "tp", None, None)),
        check_vma=False,
    )
```

```python
import functools

import jax
import jax.numpy as jnp
from jax import lax
from jax.experimental import pallas as pl
from jax.experimental.pallas import tpu as pltpu
from jax.sharding import PartitionSpec as P

HEADS = 16
EPS = 1e-06
MESH = pl.DeviceIdType.MESH
F32 = jnp.float32
BF16 = jnp.bfloat16
DMA = pltpu.SemaphoreType.DMA
PAIR = 2
CORES = 2
GAIN_ROWS = 16
WIDTH = 512
LAG_A, LAG_B = 5, 5
LAG_1, LAG_2, LAG_3, LAG_4 = 4, 4, 4, 3
DIRECT_A, DIRECT_M, DIRECT_U, DIRECT_H = 3, 2, 3, 2
HOLD, EARLY = 6, 2
FIRST = 0
CHUNKS = 1


def head_decays(count):
    index = jnp.arange(count, dtype=jnp.float32)
    return 1.0 - 2.0 ** (-1.0 - 6.0 * index / (count - 1))


def put(src, dst, send_sem, recv_sem, where):
    copy = pltpu.make_async_remote_copy(
        src_ref=src,
        dst_ref=dst,
        send_sem=send_sem,
        recv_sem=recv_sem,
        device_id=where,
        device_id_type=MESH,
    )
    copy.start()
    return copy


def landed(ref, sem):
    pltpu.make_async_copy(ref, ref, sem).wait()


def tp_gather(buf, tp, n_tp, sems):
    for d in range(1, n_tp):
        put(buf.at[tp], buf.at[tp], sems.at[0], sems.at[1], {"tp": lax.rem(tp + d, n_tp)})


def tp_scatter(src, dst, tp, n_tp, sems):
    for d in range(1, n_tp):
        peer = lax.rem(tp + d, n_tp)
        put(src.at[peer], dst.at[d - 1], sems.at[0], sems.at[1], {"tp": peer})


def square_total(squares, sq_src, sq_dst, kv, n_kv, rows, sems):
    for g in range(n_kv):
        sq_src[g] = jnp.broadcast_to(squares[g * rows : (g + 1) * rows], sq_src.shape[1:])
    for d in range(1, n_kv):
        peer = lax.rem(kv + d, n_kv)
        put(sq_src.at[peer], sq_dst.at[d - 1], sems.at[0], sems.at[1], {"kv": peer})

    def finish():
        landed(sq_dst, sems.at[1])
        total = sq_src[kv]
        for d in range(n_kv - 1):
            total = total + sq_dst[d]
        return total[:, :1]

    return finish


def send_order(s, direct):
    if s < FIRST:
        return s + direct
    return s - FIRST if s < FIRST + direct else s


class PairScatter:
    def __init__(self, kv, n_kv, rows, direct, bufs, sends, sem_a, sem_b):
        self.kv, self.n_kv, self.n_z = kv, n_kv, n_kv // PAIR
        self.z, self.y = lax.div(kv, PAIR), lax.rem(kv, PAIR)
        self.rows, self.direct = rows, direct
        self.part, self.got, self.summed, self.got2, self.got_all = bufs
        self.sends, self.sem_a, self.sem_b = sends, sem_a, sem_b

    def start(self, p, value):
        rows = self.rows
        for z in range(self.n_z):
            for y in range(PAIR):
                at = (z * PAIR + y) * rows
                self.part[p, y, z] = value[at : at + rows].astype(BF16)
        if p < self.direct:
            for d in range(1, self.n_kv):
                peer = lax.rem(self.kv + d, self.n_kv)
                put(
                    self.part.at[p, lax.rem(peer, PAIR), lax.div(peer, PAIR)],
                    self.got_all.at[p, d - 1],
                    self.sends.at[2],
                    self.sem_b.at[p],
                    {"kv": peer},
                )
            return
        other = 1 - self.y
        put(
            self.part.at[p, other],
            self.got.at[p],
            self.sends.at[0],
            self.sem_a.at[p],
            {"kv": self.z * PAIR + other},
        )

    def middle(self, p):
        if p < self.direct:
            return
        landed(self.got.at[p], self.sem_a.at[p])
        self.summed[p] = (self.part[p, self.y].astype(F32) + self.got[p].astype(F32)).astype(BF16)
        for d in range(1, self.n_z):
            peer = lax.rem(self.z + d, self.n_z)
            put(
                self.summed.at[p, peer],
                self.got2.at[p, d - 1],
                self.sends.at[1],
                self.sem_b.at[p],
                {"kv": peer * PAIR + self.y},
            )

    def finish(self, p):
        if p < self.direct:
            landed(self.got_all.at[p], self.sem_b.at[p])
            own, got = self.part[p, self.y, self.z], self.got_all
        else:
            landed(self.got2.at[p], self.sem_b.at[p])
            own, got = self.summed[p, self.z], self.got2
        total = own.astype(F32)
        for d in range(got.shape[1]):
            total = total + got[p, d].astype(F32)
        return total

    def drain(self):
        rest = pl.ds(self.direct, self.got.shape[0] - self.direct)
        landed(self.got.at[rest], self.sends.at[0])
        landed(self.got2.at[rest], self.sends.at[1])
        if self.direct:
            landed(self.got_all.at[pl.ds(0, self.direct)], self.sends.at[2])


class PairGather:
    def __init__(self, kv, n_kv, direct, buf, like, sends, sem_z, sem_y):
        self.kv, self.n_kv, self.n_z = kv, n_kv, n_kv // PAIR
        self.z, self.y = lax.div(kv, PAIR), lax.rem(kv, PAIR)
        self.relayed, self.direct = buf.shape[0] - direct, direct
        self.buf, self.like = buf, like
        self.sends, self.sem_z, self.sem_y = sends, sem_z, sem_y

    def start(self, p):
        own = self.buf.at[p, self.z, self.y]
        if p >= self.relayed:
            for d in range(1, self.n_kv):
                peer = {"kv": lax.rem(self.kv + d, self.n_kv)}
                put(own, own, self.sends.at[2], self.sem_z.at[p], peer)
            return
        for d in range(1, self.n_z):
            peer = lax.rem(self.z + d, self.n_z)
            put(own, own, self.sends.at[0], self.sem_z.at[p], {"kv": peer * PAIR + self.y})

    def relay(self, p):
        if p >= self.relayed:
            return
        landed(self.buf.at[p, pl.ds(0, self.n_z - 1), 0], self.sem_z.at[p])
        put(
            self.buf.at[p, :, self.y],
            self.buf.at[p, :, self.y],
            self.sends.at[1],
            self.sem_y.at[p],
            {"kv": self.z * PAIR + 1 - self.y},
        )

    def finish(self, p):
        if p >= self.relayed:
            landed(self.like.at[0], self.sem_z.at[p])
        else:
            landed(self.buf.at[p, :, 0], self.sem_y.at[p])
        blocks = [
            self.buf[p, z, y].astype(F32) for z in range(self.n_z) for y in range(PAIR)
        ]
        return jnp.concatenate(blocks, axis=0).astype(BF16)

    def drain(self):
        rest = pl.ds(0, self.relayed)
        landed(self.buf.at[rest, pl.ds(0, self.n_z - 1), 0], self.sends.at[0])
        landed(self.buf.at[rest, :, 0], self.sends.at[1])
        if self.direct:
            landed(self.like.at[pl.ds(0, self.direct)], self.sends.at[2])


def fused_kernel(sizes, rate_ref, x_hbm, mg_hbm, cg_hbm, *refs):
    n_kv, n_tp, rows, width, dk, dv, heads, dim = sizes
    (qw_hbm, kw_hbm, vw_hbm, gw_hbm, ow_hbm, up_hbm, down_hbm, old_hbm) = refs[:8]
    (out_ref, held) = refs[8:10]
    (pack, gain_in, qw, kw, vw, gw, ow, up, down) = refs[10:19]
    bufs, bufs_u, refs = refs[19:24], refs[24:29], refs[29:]
    (sq_src, sq_dst, sq_src2, sq_dst2, mixes, hid, ret, acc, keys, vals) = refs[:10]
    (pair_own, pair_got, chip, far, mids, ends, got_ends) = refs[10:17]
    (w_sem, s_sem, in_sem, t_sem, sq_sem, sq_sem2) = refs[17:23]
    (sems, sems_u, sems_m, sems_h) = refs[23:26], refs[26:29], refs[29:32], refs[32:35]
    (c_sem, far_sem, f_sem) = refs[35:38]
    kv, tp = lax.axis_index("kv"), lax.axis_index("tp")
    z, y = lax.div(kv, PAIR), lax.rem(kv, PAIR)
    n_x = n_tp // CORES
    cx, core = lax.div(tp, CORES), lax.rem(tp, CORES)
    batch, block = x_hbm.shape
    loads = {}

    def load(name, src, dst, sem):
        loads[name] = pltpu.make_async_copy(src, dst, sem)
        loads[name].start()

    barrier = pltpu.get_barrier_semaphore()
    for d in range(1, n_kv):
        pl.semaphore_signal(
            barrier, inc=1, device_id={"kv": lax.rem(kv + d, n_kv)}, device_id_type=MESH
        )
    for d in range(1, n_tp):
        pl.semaphore_signal(
            barrier, inc=1, device_id={"tp": lax.rem(tp + d, n_tp)}, device_id_type=MESH
        )
    load("x", x_hbm, pack.at[tp, pl.ds(0, batch)], in_sem.at[0])
    load("mg", mg_hbm, gain_in.at[0], in_sem.at[1])
    load("cg", cg_hbm, gain_in.at[1], in_sem.at[2])
    for name in ("x", "mg", "cg"):
        loads[name].wait()
    for i, (name, src, dst) in enumerate(
        [("q", qw_hbm, qw), ("k", kw_hbm, kw), ("v", vw_hbm, vw), ("g", gw_hbm, gw)]
    ):
        load(name, src, dst, w_sem.at[i])
    for i in range(2):
        gain = jnp.broadcast_to(gain_in[i].astype(F32), (GAIN_ROWS, block))
        pack[tp, batch + i * GAIN_ROWS : batch + (i + 1) * GAIN_ROWS] = gain.astype(BF16)
    pl.semaphore_wait(barrier, n_tp + n_kv - 2)
    tp_gather(pack, tp, n_tp, t_sem)
    load("old", old_hbm, held, s_sem)
    landed(pack.at[pl.ds(0, n_tp - 1)], t_sem.at[1])

    def normalise(stream, row):
        parts = [
            (stream[t] * pack[t, row : row + GAIN_ROWS][:1].astype(F32)).astype(BF16)
            for t in range(n_tp)
        ]
        return jnp.concatenate(parts, axis=1)

    def squares_of(stream):
        return sum(jnp.sum(s * s, axis=1, keepdims=True) for s in stream)

    stream = [pack[t, :batch].astype(F32) for t in range(n_tp)]
    normed = normalise(stream, batch)
    sq_total = square_total(squares_of(stream), sq_src, sq_dst, kv, n_kv, rows, sq_sem)
    scatter = PairScatter(kv, n_kv, rows, DIRECT_A, bufs, *sems)
    mix_gather = PairGather(kv, n_kv, DIRECT_M, mixes, bufs[4], *sems_m)

    ready = set()

    def project(p):
        h, kind = divmod(p, 3)
        for name in (("q", "k"), ("v",), ("g",))[kind]:
            if name not in ready:
                loads[name].wait()
                ready.add(name)
        if kind == 0:
            cols = slice(h * dk, (h + 1) * dk)
            return jnp.concatenate(
                [
                    jnp.dot(normed, qw[:, cols], preferred_element_type=F32),
                    jnp.dot(normed, kw[:, cols], preferred_element_type=F32),
                ],
                axis=1,
            )
        w = (vw, gw)[kind - 1]
        return jnp.dot(normed, w[:, h * dv : (h + 1) * dv], preferred_element_type=F32)

    def retain(h, query, key, value):
        columns = query.T
        step = min(dk, 64)
        for s in range(rows):
            total = jnp.zeros((8, dv), F32)
            for r in range(0, dk, step):
                term = columns[r : r + step, s : s + 1] * held[s, h, r : r + step]
                total = total + jnp.sum(term.reshape(step // 8, 8, dv), axis=0)
            ret[s : s + 1] = jnp.sum(total, axis=0, keepdims=True)
        out = rate_ref[h] * ret[...] + jnp.sum(query * key, axis=1, keepdims=True) * value
        ret[...] = out * lax.rsqrt(jnp.mean(out * out, axis=1, keepdims=True) + EPS)

    def update(h):
        columns, value = keys[h].T, vals[h]
        step = min(dk, 64)
        for s in range(rows):
            line = value[s : s + 1]
            for r in range(0, dk, step):
                term = columns[r : r + step, s : s + 1] * line
                held[s, h, r : r + step] = rate_ref[h] * held[s, h, r : r + step] + term

    def attend(h):
        if h == 0:
            loads["ow"].wait()
        term = jnp.dot(
            mix_gather.finish(h), ow[h * dv : (h + 1) * dv], preferred_element_type=F32
        )
        acc[...] = term if h == 0 else acc[...] + term

    pieces = 3 * heads
    scale, values, pending = None, {}, []
    for s in range(pieces + LAG_A + LAG_B):
        if s < pieces:
            first = send_order(s, DIRECT_A)
            scatter.start(first, project(first))
        if s == 0:
            load("ow", ow_hbm, ow, w_sem.at[4])
            load("up", up_hbm, up, w_sem.at[5])
            load("down", down_hbm, down, w_sem.at[6])
        p = s - LAG_A
        if 0 <= p < pieces:
            scatter.middle(p)
        p = p - LAG_B
        if 0 <= p < pieces:
            if p == 0:
                scale = lax.rsqrt(sq_total() / dim + EPS)
            h, kind = divmod(p, 3)
            total = scatter.finish(p) * scale
            if kind == 0:
                query, key = total[:, :dk], total[:, dk:] * dk ** (-0.5)
                keys[h] = key
                values["q"], values["k"] = query, key
            elif kind == 1:
                vals[h] = total
                if h == 0:
                    loads["old"].wait()
                retain(h, values["q"], values["k"], total)
            else:
                mixes[h, z, y] = (jax.nn.silu(total) * ret[...]).astype(BF16)
                if h < heads - 1:
                    pending.append(h)
                else:
                    mix_gather.start(h)
            if p >= HOLD:
                for g in pending:
                    mix_gather.start(g)
                pending = []
    for h in range(heads - 1):
        mix_gather.relay(h)
    for h in range(min(EARLY, heads - 1)):
        update(h)
    for h in range(heads):
        attend(h)

    half = pair_own.shape[1] // 2
    pair_own[...] = acc[...].astype(BF16)
    pair_copy = put(
        pair_own, pair_got, c_sem.at[0], c_sem.at[1], {"tp": cx * CORES + 1 - core}
    )
    pair_copy.wait_recv()
    both = pair_own[...].astype(F32) + pair_got[...].astype(F32)
    for j in range(CORES):
        chip[j] = both[:, j * half : (j + 1) * half].astype(BF16)
    for d in range(1, n_x):
        for rel in range(CORES):
            peer = lax.rem(cx + d, n_x) * CORES + lax.rem(core + rel, CORES)
            put(
                chip.at[core],
                far.at[d - 1, rel],
                far_sem.at[0],
                far_sem.at[1],
                {"tp": peer},
            )
    for h in range(min(EARLY, heads - 1), heads):
        update(h)
    landed(far, far_sem.at[1])
    sums = []
    for j in range(CORES):
        total = chip[j].astype(F32)
        for d in range(n_x - 1):
            total = total + far[d, lax.rem(core + j, CORES)].astype(F32)
        sums.append(total)
    attention = jnp.concatenate(sums, axis=1)
    for t in range(n_tp):
        mids[t] = (
            pack[t, :batch].astype(F32) + attention[:, t * block : (t + 1) * block]
        ).astype(BF16)
    stream = [mids[t].astype(F32) for t in range(n_tp)]
    normed_mid = normalise(stream, batch + GAIN_ROWS)
    sq_total2 = square_total(squares_of(stream), sq_src2, sq_dst2, kv, n_kv, rows, sq_sem2)
    lift = PairScatter(kv, n_kv, rows, DIRECT_U, bufs_u, *sems_u)
    gather = PairGather(kv, n_kv, DIRECT_H, hid, bufs_u[4], *sems_h)
    count = up.shape[1] // width
    loads["up"].wait()
    scale2 = None
    for s in range(count + LAG_1 + LAG_2 + LAG_3 + LAG_4):
        if s < count:
            first = send_order(s, DIRECT_U)
            w = up[:, first * width : (first + 1) * width]
            lift.start(first, jnp.dot(normed_mid, w, preferred_element_type=F32))
        p = s - LAG_1
        if 0 <= p < count:
            lift.middle(p)
        p = p - LAG_2
        if 0 <= p < count:
            if p == 0:
                scale2 = lax.rsqrt(sq_total2() / dim + EPS)
            lifted = lift.finish(p) * scale2
            hid[p, z, y] = jnp.square(jnp.maximum(lifted, 0.0)).astype(BF16)
            gather.start(p)
        p = p - LAG_3
        if 0 <= p < count:
            gather.relay(p)
        p = p - LAG_4
        if 0 <= p < count:
            if p == 0:
                loads["down"].wait()
            w = down[p * width : (p + 1) * width]
            term = jnp.dot(gather.finish(p), w, preferred_element_type=F32)
            acc[...] = term if p == 0 else acc[...] + term
    for t in range(n_tp):
        ends[t] = acc[:, t * block : (t + 1) * block].astype(BF16)
    tp_scatter(ends, got_ends, tp, n_tp, f_sem)
    landed(got_ends, f_sem.at[1])
    lowered = ends[tp].astype(F32)
    for d in range(n_tp - 1):
        lowered = lowered + got_ends[d].astype(F32)
    out_ref[...] = (mids[tp].astype(F32) + lowered).astype(BF16)
    for group in (scatter, mix_gather, lift, gather):
        group.drain()
    pair_copy.wait_send()
    landed(pack.at[pl.ds(0, n_tp - 1)], t_sem.at[0])
    landed(sq_dst, sq_sem.at[0])
    landed(sq_dst2, sq_sem2.at[0])
    landed(far, far_sem.at[0])
    landed(got_ends, f_sem.at[0])


def write_kernel(act_ref, state_ref, act_out, state_out, act_sem, sem):
    copies = [pltpu.make_async_copy(act_ref, act_out, act_sem)]
    for s in range(state_ref.shape[0]):
        for h in range(CHUNKS):
            n = state_ref.shape[1] // CHUNKS
            part = (s, pl.ds(h * n, n))
            copies.append(
                pltpu.make_async_copy(state_ref.at[part], state_out.at[part], sem.at[s, h])
            )
    for copy in copies:
        copy.start()
    for copy in copies:
        copy.wait()


def in_hbm(a):
    return pltpu.with_memory_space_constraint(a, pltpu.HBM)


VM = pl.BlockSpec(memory_space=pltpu.VMEM)
SM = pl.BlockSpec(memory_space=pltpu.SMEM)
ANY = pl.BlockSpec(memory_space=pltpu.HBM)


def scatter_scratch(count, n_kv, rows, width, direct):
    n_z = n_kv // PAIR
    return [
        pltpu.VMEM((count, PAIR, n_z, rows, width), BF16),
        pltpu.VMEM((count, n_z, rows, width), BF16),
        pltpu.VMEM((count, n_z, rows, width), BF16),
        pltpu.VMEM((count, n_z - 1, rows, width), BF16),
        pltpu.VMEM((max(direct, 1), n_kv - 1, rows, width), BF16),
    ]


def fused_device(n_kv, n_tp, x, mg, cg, qw, kw, vw, gw, ow, uw, dw, state):
    seqs, heads, dk, dv = state.shape
    batch, block = x.shape
    dim = block * n_kv * n_tp
    n_z, n_x = n_kv // PAIR, n_tp // CORES
    depth, cols = qw.shape[0], ow.shape[1]
    width = min(WIDTH, uw.shape[1])
    count, pieces = uw.shape[1] // width, 3 * heads
    rates = lax.dynamic_slice_in_dim(
        head_decays(HEADS), lax.axis_index("tp") * heads, heads, 0
    )
    elements = sum(w.size for w in (qw, kw, vw, gw, ow, uw, dw))
    out, held = pl.pallas_call(
        functools.partial(fused_kernel, (n_kv, n_tp, seqs, width, dk, dv, heads, dim)),
        out_shape=[
            jax.ShapeDtypeStruct((batch, block), BF16),
            pltpu.VMEM(state.shape, F32),
        ],
        in_specs=[SM] + [ANY] * 11,
        out_specs=[VM] * 2,
        scratch_shapes=[
            pltpu.VMEM((n_tp, batch + 2 * GAIN_ROWS, block), BF16),
            pltpu.VMEM((2, 1, block), BF16),
            *[pltpu.VMEM(w.shape, BF16) for w in (qw, kw, vw, gw, ow, uw, dw)],
            *scatter_scratch(pieces, n_kv, seqs, dv, max(DIRECT_A, DIRECT_M)),
            *scatter_scratch(count, n_kv, seqs, width, max(DIRECT_U, DIRECT_H)),
            pltpu.VMEM((n_kv, seqs, 128), F32),
            pltpu.VMEM((n_kv - 1, seqs, 128), F32),
            pltpu.VMEM((n_kv, seqs, 128), F32),
            pltpu.VMEM((n_kv - 1, seqs, 128), F32),
            pltpu.VMEM((heads, n_z, PAIR, seqs, dv), BF16),
            pltpu.VMEM((count, n_z, PAIR, seqs, width), BF16),
            pltpu.VMEM((seqs, dv), F32),
            pltpu.VMEM((batch, cols), F32),
            pltpu.VMEM((heads, seqs, dk), F32),
            pltpu.VMEM((heads, seqs, dv), F32),
            pltpu.VMEM((batch, cols), BF16),
            pltpu.VMEM((batch, cols), BF16),
            pltpu.VMEM((CORES, batch, cols // CORES), BF16),
            pltpu.VMEM((max(n_x - 1, 1), CORES, batch, cols // CORES), BF16),
            pltpu.VMEM((n_tp, batch, block), BF16),
            pltpu.VMEM((n_tp, batch, block), BF16),
            pltpu.VMEM((n_tp - 1, batch, block), BF16),
            DMA((7,)),
            DMA,
            DMA((3,)),
            *[DMA((2,))] * 3,
            *[DMA((3,)), *[DMA((pieces,))] * 2],
            *[DMA((3,)), *[DMA((count,))] * 2],
            *[DMA((3,)), *[DMA((heads,))] * 2],
            *[DMA((3,)), *[DMA((count,))] * 2],
            *[DMA((2,))] * 3,
        ],
        compiler_params=pltpu.CompilerParams(
            collective_id=0, has_side_effects=True, vmem_limit_bytes=26 * 2**20
        ),
        cost_estimate=pl.CostEstimate(
            flops=2 * batch * elements,
            bytes_accessed=2 * elements + 4 * state.size,
            transcendentals=0,
        ),
        name="fused",
    )(
        rates,
        *[in_hbm(a) for a in (x, mg.reshape(1, block), cg.reshape(1, block))],
        *[in_hbm(a) for a in (qw, kw, vw, gw, ow, uw, dw, state)],
    )
    return pl.pallas_call(
        write_kernel,
        out_shape=[pltpu.HBM((batch, block), BF16), pltpu.HBM(state.shape, F32)],
        in_specs=[VM, VM],
        out_specs=[ANY, ANY],
        scratch_shapes=[DMA, DMA((seqs, CHUNKS))],
        compiler_params=pltpu.CompilerParams(vmem_limit_bytes=2**20),
        cost_estimate=pl.CostEstimate(
            flops=state.size, bytes_accessed=4 * state.size, transcendentals=0
        ),
        name="write",
    )(out, held)


def solution(mesh):
    return jax.shard_map(
        functools.partial(fused_device, mesh.shape["kv"], mesh.shape["tp"]),
        mesh=mesh,
        in_specs=(
            P(None, ("kv", "tp")),
            P(("kv", "tp")),
            P(("kv", "tp")),
            P("kv", "tp"),
            P("kv", "tp"),
            P("kv", "tp"),
            P("kv", "tp"),
            P("tp", "kv"),
            P("kv", "tp"),
            P("tp", "kv"),
            P("kv", "tp", None, None),
        ),
        out_specs=(P(None, ("kv", "tp")), P("kv", "tp", None, None)),
        check_vma=False,
    )
```

```python
import functools

import jax
import jax.numpy as jnp
from jax import lax
from jax.experimental import pallas as pl
from jax.experimental.pallas import tpu as pltpu
from jax.sharding import PartitionSpec as P

HEADS = 16
EPS = 1e-06
MESH = pl.DeviceIdType.MESH
F32 = jnp.float32
BF16 = jnp.bfloat16
DMA = pltpu.SemaphoreType.DMA
PAIR = 2
CORES = 2
GAIN_ROWS = 16
WIDTH = 512
LAG_A, LAG_B = 5, 5
LAG_1, LAG_2, LAG_3, LAG_4 = 4, 4, 4, 3
DIRECT_M, DIRECT_H = 2, 2
ALONG_A, ALONG_U = (3, 4), (3, 4)
SEND = (0, 3, 4, 1, 2)
FOLD = (0, 1, 2, 3, 5, 4)
HOLD, EARLY = 6, 2
CHUNKS = 1


def head_decays(count):
    index = jnp.arange(count, dtype=jnp.float32)
    return 1.0 - 2.0 ** (-1.0 - 6.0 * index / (count - 1))


def put(src, dst, send_sem, recv_sem, where):
    copy = pltpu.make_async_remote_copy(
        src_ref=src,
        dst_ref=dst,
        send_sem=send_sem,
        recv_sem=recv_sem,
        device_id=where,
        device_id_type=MESH,
    )
    copy.start()
    return copy


def landed(ref, sem):
    pltpu.make_async_copy(ref, ref, sem).wait()


def tp_gather(buf, tp, n_tp, sems):
    for d in range(1, n_tp):
        put(buf.at[tp], buf.at[tp], sems.at[0], sems.at[1], {"tp": lax.rem(tp + d, n_tp)})


def tp_scatter(src, dst, tp, n_tp, sems):
    for d in range(1, n_tp):
        peer = lax.rem(tp + d, n_tp)
        put(src.at[peer], dst.at[d - 1], sems.at[0], sems.at[1], {"tp": peer})


def square_total(squares, sq_src, sq_dst, kv, n_kv, rows, sems):
    for g in range(n_kv):
        sq_src[g] = jnp.broadcast_to(squares[g * rows : (g + 1) * rows], sq_src.shape[1:])
    for d in range(1, n_kv):
        peer = lax.rem(kv + d, n_kv)
        put(sq_src.at[peer], sq_dst.at[d - 1], sems.at[0], sems.at[1], {"kv": peer})

    def finish():
        landed(sq_dst, sems.at[1])
        total = sq_src[kv]
        for d in range(n_kv - 1):
            total = total + sq_dst[d]
        return total[:, :1]

    return finish


def in_order(order, s):
    return order[s] if s < len(order) else s


class PairScatter:
    def __init__(self, kv, n_kv, rows, along, bufs, sends, sem_a, sem_b):
        self.kv, self.n_kv, self.n_z = kv, n_kv, n_kv // PAIR
        self.z, self.y = lax.div(kv, PAIR), lax.rem(kv, PAIR)
        self.rows, self.other = rows, {"kv": self.z * PAIR + 1 - self.y}
        self.part, self.got, self.summed, self.got2, self.got_all, self.kept = bufs
        self.along = {p: i for i, p in enumerate(along) if p < self.got.shape[0]}
        self.sends, self.sem_a, self.sem_b = sends, sem_a, sem_b

    def start(self, p, value):
        rows = self.rows
        for z in range(self.n_z):
            for y in range(PAIR):
                at = (z * PAIR + y) * rows
                self.part[p, y, z] = value[at : at + rows].astype(BF16)
        if p in self.along:
            for d in range(1, self.n_z):
                peer = lax.rem(self.z + d, self.n_z)
                put(
                    self.part.at[p, :, peer],
                    self.got_all.at[self.along[p], pl.ds((d - 1) * PAIR, PAIR)],
                    self.sends.at[2],
                    self.sem_b.at[p],
                    {"kv": peer * PAIR + self.y},
                )
            return
        put(
            self.part.at[p, 1 - self.y],
            self.got.at[p],
            self.sends.at[0],
            self.sem_a.at[p],
            self.other,
        )

    def middle(self, p):
        if p in self.along:
            at, count = self.along[p], (self.n_z - 1) * PAIR
            landed(self.got_all.at[at, pl.ds(0, count)], self.sem_b.at[p])

            def total(y):
                value = self.part[p, y, self.z].astype(F32)
                for d in range(0, count, PAIR):
                    value = value + self.got_all[at, d + y].astype(F32)
                return value

            self.summed[p, 0] = total(1 - self.y).astype(BF16)
            self.kept[at] = total(self.y)
            put(
                self.summed.at[p, 0],
                self.got.at[p, 0],
                self.sends.at[3],
                self.sem_a.at[p],
                self.other,
            )
            return
        landed(self.got.at[p], self.sem_a.at[p])
        self.summed[p] = (self.part[p, self.y].astype(F32) + self.got[p].astype(F32)).astype(BF16)
        for d in range(1, self.n_z):
            peer = lax.rem(self.z + d, self.n_z)
            put(
                self.summed.at[p, peer],
                self.got2.at[p, d - 1],
                self.sends.at[1],
                self.sem_b.at[p],
                {"kv": peer * PAIR + self.y},
            )

    def finish(self, p):
        if p in self.along:
            landed(self.got.at[p, 0], self.sem_a.at[p])
            return self.kept[self.along[p]] + self.got[p, 0].astype(F32)
        landed(self.got2.at[p], self.sem_b.at[p])
        total = self.summed[p, self.z].astype(F32)
        for d in range(self.n_z - 1):
            total = total + self.got2[p, d].astype(F32)
        return total

    def drain(self):
        n = len(self.along)
        rest = pl.ds(0, self.got.shape[0] - n)
        landed(self.got.at[rest], self.sends.at[0])
        landed(self.got2.at[rest], self.sends.at[1])
        if n:
            blocks = self.got_all.at[pl.ds(0, n), pl.ds(0, (self.n_z - 1) * PAIR)]
            landed(blocks, self.sends.at[2])
            landed(self.got.at[pl.ds(0, n), 0], self.sends.at[3])


class PairGather:
    def __init__(self, kv, n_kv, direct, buf, like, sends, sem_z, sem_y):
        self.kv, self.n_kv, self.n_z = kv, n_kv, n_kv // PAIR
        self.z, self.y = lax.div(kv, PAIR), lax.rem(kv, PAIR)
        self.relayed, self.direct = buf.shape[0] - direct, direct
        self.buf, self.like = buf, like
        self.sends, self.sem_z, self.sem_y = sends, sem_z, sem_y

    def start(self, p):
        own = self.buf.at[p, self.z, self.y]
        if p >= self.relayed:
            for d in range(1, self.n_kv):
                peer = {"kv": lax.rem(self.kv + d, self.n_kv)}
                put(own, own, self.sends.at[2], self.sem_z.at[p], peer)
            return
        for d in range(1, self.n_z):
            peer = lax.rem(self.z + d, self.n_z)
            put(own, own, self.sends.at[0], self.sem_z.at[p], {"kv": peer * PAIR + self.y})

    def relay(self, p):
        if p >= self.relayed:
            return
        landed(self.buf.at[p, pl.ds(0, self.n_z - 1), 0], self.sem_z.at[p])
        put(
            self.buf.at[p, :, self.y],
            self.buf.at[p, :, self.y],
            self.sends.at[1],
            self.sem_y.at[p],
            {"kv": self.z * PAIR + 1 - self.y},
        )

    def finish(self, p):
        if p >= self.relayed:
            landed(self.like.at[0], self.sem_z.at[p])
        else:
            landed(self.buf.at[p, :, 0], self.sem_y.at[p])
        blocks = [
            self.buf[p, z, y].astype(F32) for z in range(self.n_z) for y in range(PAIR)
        ]
        return jnp.concatenate(blocks, axis=0).astype(BF16)

    def drain(self):
        rest = pl.ds(0, self.relayed)
        landed(self.buf.at[rest, pl.ds(0, self.n_z - 1), 0], self.sends.at[0])
        landed(self.buf.at[rest, :, 0], self.sends.at[1])
        if self.direct:
            landed(self.like.at[pl.ds(0, self.direct)], self.sends.at[2])


def fused_kernel(sizes, rate_ref, x_hbm, mg_hbm, cg_hbm, *refs):
    n_kv, n_tp, rows, width, dk, dv, heads, dim = sizes
    (qw_hbm, kw_hbm, vw_hbm, gw_hbm, ow_hbm, up_hbm, down_hbm, old_hbm) = refs[:8]
    (out_ref, held) = refs[8:10]
    (pack, gain_in, qw, kw, vw, gw, ow, up, down) = refs[10:19]
    bufs, bufs_u, refs = refs[19:25], refs[25:31], refs[31:]
    (sq_src, sq_dst, sq_src2, sq_dst2, mixes, hid, ret, acc, keys, vals) = refs[:10]
    (pair_own, pair_got, chip, far, mids, ends, got_ends) = refs[10:17]
    (w_sem, s_sem, in_sem, t_sem, sq_sem, sq_sem2) = refs[17:23]
    (sems, sems_u, sems_m, sems_h) = refs[23:26], refs[26:29], refs[29:32], refs[32:35]
    (c_sem, far_sem, f_sem) = refs[35:38]
    kv, tp = lax.axis_index("kv"), lax.axis_index("tp")
    z, y = lax.div(kv, PAIR), lax.rem(kv, PAIR)
    n_x = n_tp // CORES
    cx, core = lax.div(tp, CORES), lax.rem(tp, CORES)
    batch, block = x_hbm.shape
    loads = {}

    def load(name, src, dst, sem):
        loads[name] = pltpu.make_async_copy(src, dst, sem)
        loads[name].start()

    barrier = pltpu.get_barrier_semaphore()
    for d in range(1, n_kv):
        pl.semaphore_signal(
            barrier, inc=1, device_id={"kv": lax.rem(kv + d, n_kv)}, device_id_type=MESH
        )
    for d in range(1, n_tp):
        pl.semaphore_signal(
            barrier, inc=1, device_id={"tp": lax.rem(tp + d, n_tp)}, device_id_type=MESH
        )
    load("x", x_hbm, pack.at[tp, pl.ds(0, batch)], in_sem.at[0])
    load("mg", mg_hbm, gain_in.at[0], in_sem.at[1])
    load("cg", cg_hbm, gain_in.at[1], in_sem.at[2])
    for name in ("x", "mg", "cg"):
        loads[name].wait()
    for i, (name, src, dst) in enumerate(
        [("q", qw_hbm, qw), ("k", kw_hbm, kw), ("v", vw_hbm, vw), ("g", gw_hbm, gw)]
    ):
        load(name, src, dst, w_sem.at[i])
    for i in range(2):
        gain = jnp.broadcast_to(gain_in[i].astype(F32), (GAIN_ROWS, block))
        pack[tp, batch + i * GAIN_ROWS : batch + (i + 1) * GAIN_ROWS] = gain.astype(BF16)
    pl.semaphore_wait(barrier, n_tp + n_kv - 2)
    tp_gather(pack, tp, n_tp, t_sem)
    load("old", old_hbm, held, s_sem)
    landed(pack.at[pl.ds(0, n_tp - 1)], t_sem.at[1])

    def normalise(stream, row):
        parts = [
            (stream[t] * pack[t, row : row + GAIN_ROWS][:1].astype(F32)).astype(BF16)
            for t in range(n_tp)
        ]
        return jnp.concatenate(parts, axis=1)

    def squares_of(stream):
        return sum(jnp.sum(s * s, axis=1, keepdims=True) for s in stream)

    stream = [pack[t, :batch].astype(F32) for t in range(n_tp)]
    normed = normalise(stream, batch)
    sq_total = square_total(squares_of(stream), sq_src, sq_dst, kv, n_kv, rows, sq_sem)
    scatter = PairScatter(kv, n_kv, rows, ALONG_A, bufs, *sems)
    mix_gather = PairGather(kv, n_kv, DIRECT_M, mixes, bufs[4], *sems_m)

    ready = set()

    def project(p):
        h, kind = divmod(p, 3)
        for name in (("q", "k"), ("v",), ("g",))[kind]:
            if name not in ready:
                loads[name].wait()
                ready.add(name)
        if kind == 0:
            cols = slice(h * dk, (h + 1) * dk)
            return jnp.concatenate(
                [
                    jnp.dot(normed, qw[:, cols], preferred_element_type=F32),
                    jnp.dot(normed, kw[:, cols], preferred_element_type=F32),
                ],
                axis=1,
            )
        w = (vw, gw)[kind - 1]
        return jnp.dot(normed, w[:, h * dv : (h + 1) * dv], preferred_element_type=F32)

    def retain(h, query, key, value):
        columns = query.T
        step = min(dk, 64)
        for s in range(rows):
            total = jnp.zeros((8, dv), F32)
            for r in range(0, dk, step):
                term = columns[r : r + step, s : s + 1] * held[s, h, r : r + step]
                total = total + jnp.sum(term.reshape(step // 8, 8, dv), axis=0)
            ret[s : s + 1] = jnp.sum(total, axis=0, keepdims=True)
        out = rate_ref[h] * ret[...] + jnp.sum(query * key, axis=1, keepdims=True) * value
        ret[...] = out * lax.rsqrt(jnp.mean(out * out, axis=1, keepdims=True) + EPS)

    def update(h):
        columns, value = keys[h].T, vals[h]
        step = min(dk, 64)
        for s in range(rows):
            line = value[s : s + 1]
            for r in range(0, dk, step):
                term = columns[r : r + step, s : s + 1] * line
                held[s, h, r : r + step] = rate_ref[h] * held[s, h, r : r + step] + term

    def attend(h):
        if h == 0:
            loads["ow"].wait()
        term = jnp.dot(
            mix_gather.finish(h), ow[h * dv : (h + 1) * dv], preferred_element_type=F32
        )
        acc[...] = term if h == 0 else acc[...] + term

    pieces = 3 * heads
    scale, values, pending = None, {}, []
    for s in range(pieces + LAG_A + LAG_B):
        if s < pieces:
            first = in_order(SEND, s)
            scatter.start(first, project(first))
        if s == 0:
            load("ow", ow_hbm, ow, w_sem.at[4])
            load("up", up_hbm, up, w_sem.at[5])
            load("down", down_hbm, down, w_sem.at[6])
        p = s - LAG_A
        if 0 <= p < pieces:
            scatter.middle(in_order(FOLD, p))
        p = p - LAG_B
        if 0 <= p < pieces:
            if p == 0:
                scale = lax.rsqrt(sq_total() / dim + EPS)
            h, kind = divmod(p, 3)
            total = scatter.finish(p) * scale
            if kind == 0:
                query, key = total[:, :dk], total[:, dk:] * dk ** (-0.5)
                keys[h] = key
                values["q"], values["k"] = query, key
            elif kind == 1:
                vals[h] = total
                if h == 0:
                    loads["old"].wait()
                retain(h, values["q"], values["k"], total)
            else:
                mixes[h, z, y] = (jax.nn.silu(total) * ret[...]).astype(BF16)
                if h < heads - 1:
                    pending.append(h)
                else:
                    mix_gather.start(h)
            if p >= HOLD:
                for g in pending:
                    mix_gather.start(g)
                pending = []
    for h in range(heads - 1):
        mix_gather.relay(h)
    for h in range(min(EARLY, heads - 1)):
        update(h)
    for h in range(heads):
        attend(h)

    half = pair_own.shape[1] // 2
    pair_own[...] = acc[...].astype(BF16)
    pair_copy = put(
        pair_own, pair_got, c_sem.at[0], c_sem.at[1], {"tp": cx * CORES + 1 - core}
    )
    pair_copy.wait_recv()
    both = pair_own[...].astype(F32) + pair_got[...].astype(F32)
    for j in range(CORES):
        chip[j] = both[:, j * half : (j + 1) * half].astype(BF16)
    for d in range(1, n_x):
        for rel in range(CORES):
            peer = lax.rem(cx + d, n_x) * CORES + lax.rem(core + rel, CORES)
            put(
                chip.at[core],
                far.at[d - 1, rel],
                far_sem.at[0],
                far_sem.at[1],
                {"tp": peer},
            )
    for h in range(min(EARLY, heads - 1), heads):
        update(h)
    landed(far, far_sem.at[1])
    sums = []
    for j in range(CORES):
        total = chip[j].astype(F32)
        for d in range(n_x - 1):
            total = total + far[d, lax.rem(core + j, CORES)].astype(F32)
        sums.append(total)
    attention = jnp.concatenate(sums, axis=1)
    for t in range(n_tp):
        mids[t] = (
            pack[t, :batch].astype(F32) + attention[:, t * block : (t + 1) * block]
        ).astype(BF16)
    stream = [mids[t].astype(F32) for t in range(n_tp)]
    normed_mid = normalise(stream, batch + GAIN_ROWS)
    sq_total2 = square_total(squares_of(stream), sq_src2, sq_dst2, kv, n_kv, rows, sq_sem2)
    lift = PairScatter(kv, n_kv, rows, ALONG_U, bufs_u, *sems_u)
    gather = PairGather(kv, n_kv, DIRECT_H, hid, bufs_u[4], *sems_h)
    count = up.shape[1] // width
    loads["up"].wait()
    scale2 = None
    for s in range(count + LAG_1 + LAG_2 + LAG_3 + LAG_4):
        if s < count:
            first = in_order(SEND if count > 5 else (), s)
            w = up[:, first * width : (first + 1) * width]
            lift.start(first, jnp.dot(normed_mid, w, preferred_element_type=F32))
        p = s - LAG_1
        if 0 <= p < count:
            lift.middle(in_order(FOLD if count > 5 else (), p))
        p = p - LAG_2
        if 0 <= p < count:
            if p == 0:
                scale2 = lax.rsqrt(sq_total2() / dim + EPS)
            lifted = lift.finish(p) * scale2
            hid[p, z, y] = jnp.square(jnp.maximum(lifted, 0.0)).astype(BF16)
            gather.start(p)
        p = p - LAG_3
        if 0 <= p < count:
            gather.relay(p)
        p = p - LAG_4
        if 0 <= p < count:
            if p == 0:
                loads["down"].wait()
            w = down[p * width : (p + 1) * width]
            term = jnp.dot(gather.finish(p), w, preferred_element_type=F32)
            acc[...] = term if p == 0 else acc[...] + term
    for t in range(n_tp):
        ends[t] = acc[:, t * block : (t + 1) * block].astype(BF16)
    tp_scatter(ends, got_ends, tp, n_tp, f_sem)
    landed(got_ends, f_sem.at[1])
    lowered = ends[tp].astype(F32)
    for d in range(n_tp - 1):
        lowered = lowered + got_ends[d].astype(F32)
    out_ref[...] = (mids[tp].astype(F32) + lowered).astype(BF16)
    for group in (scatter, mix_gather, lift, gather):
        group.drain()
    pair_copy.wait_send()
    landed(pack.at[pl.ds(0, n_tp - 1)], t_sem.at[0])
    landed(sq_dst, sq_sem.at[0])
    landed(sq_dst2, sq_sem2.at[0])
    landed(far, far_sem.at[0])
    landed(got_ends, f_sem.at[0])


def write_kernel(act_ref, state_ref, act_out, state_out, act_sem, sem):
    copies = [pltpu.make_async_copy(act_ref, act_out, act_sem)]
    for s in range(state_ref.shape[0]):
        for h in range(CHUNKS):
            n = state_ref.shape[1] // CHUNKS
            part = (s, pl.ds(h * n, n))
            copies.append(
                pltpu.make_async_copy(state_ref.at[part], state_out.at[part], sem.at[s, h])
            )
    for copy in copies:
        copy.start()
    for copy in copies:
        copy.wait()


def in_hbm(a):
    return pltpu.with_memory_space_constraint(a, pltpu.HBM)


VM = pl.BlockSpec(memory_space=pltpu.VMEM)
SM = pl.BlockSpec(memory_space=pltpu.SMEM)
ANY = pl.BlockSpec(memory_space=pltpu.HBM)


def scatter_scratch(count, n_kv, rows, width, direct):
    n_z = n_kv // PAIR
    return [
        pltpu.VMEM((count, PAIR, n_z, rows, width), BF16),
        pltpu.VMEM((count, n_z, rows, width), BF16),
        pltpu.VMEM((count, n_z, rows, width), BF16),
        pltpu.VMEM((count, n_z - 1, rows, width), BF16),
        pltpu.VMEM((max(direct, 1), n_kv - 1, rows, width), BF16),
        pltpu.VMEM((max(direct, 1), rows, width), F32),
    ]


def fused_device(n_kv, n_tp, x, mg, cg, qw, kw, vw, gw, ow, uw, dw, state):
    seqs, heads, dk, dv = state.shape
    batch, block = x.shape
    dim = block * n_kv * n_tp
    n_z, n_x = n_kv // PAIR, n_tp // CORES
    depth, cols = qw.shape[0], ow.shape[1]
    width = min(WIDTH, uw.shape[1])
    count, pieces = uw.shape[1] // width, 3 * heads
    rates = lax.dynamic_slice_in_dim(
        head_decays(HEADS), lax.axis_index("tp") * heads, heads, 0
    )
    elements = sum(w.size for w in (qw, kw, vw, gw, ow, uw, dw))
    out, held = pl.pallas_call(
        functools.partial(fused_kernel, (n_kv, n_tp, seqs, width, dk, dv, heads, dim)),
        out_shape=[
            jax.ShapeDtypeStruct((batch, block), BF16),
            pltpu.VMEM(state.shape, F32),
        ],
        in_specs=[SM] + [ANY] * 11,
        out_specs=[VM] * 2,
        scratch_shapes=[
            pltpu.VMEM((n_tp, batch + 2 * GAIN_ROWS, block), BF16),
            pltpu.VMEM((2, 1, block), BF16),
            *[pltpu.VMEM(w.shape, BF16) for w in (qw, kw, vw, gw, ow, uw, dw)],
            *scatter_scratch(pieces, n_kv, seqs, dv, max(len(ALONG_A), DIRECT_M)),
            *scatter_scratch(count, n_kv, seqs, width, max(len(ALONG_U), DIRECT_H)),
            pltpu.VMEM((n_kv, seqs, 128), F32),
            pltpu.VMEM((n_kv - 1, seqs, 128), F32),
            pltpu.VMEM((n_kv, seqs, 128), F32),
            pltpu.VMEM((n_kv - 1, seqs, 128), F32),
            pltpu.VMEM((heads, n_z, PAIR, seqs, dv), BF16),
            pltpu.VMEM((count, n_z, PAIR, seqs, width), BF16),
            pltpu.VMEM((seqs, dv), F32),
            pltpu.VMEM((batch, cols), F32),
            pltpu.VMEM((heads, seqs, dk), F32),
            pltpu.VMEM((heads, seqs, dv), F32),
            pltpu.VMEM((batch, cols), BF16),
            pltpu.VMEM((batch, cols), BF16),
            pltpu.VMEM((CORES, batch, cols // CORES), BF16),
            pltpu.VMEM((max(n_x - 1, 1), CORES, batch, cols // CORES), BF16),
            pltpu.VMEM((n_tp, batch, block), BF16),
            pltpu.VMEM((n_tp, batch, block), BF16),
            pltpu.VMEM((n_tp - 1, batch, block), BF16),
            DMA((7,)),
            DMA,
            DMA((3,)),
            *[DMA((2,))] * 3,
            *[DMA((4,)), *[DMA((pieces,))] * 2],
            *[DMA((4,)), *[DMA((count,))] * 2],
            *[DMA((3,)), *[DMA((heads,))] * 2],
            *[DMA((3,)), *[DMA((count,))] * 2],
            *[DMA((2,))] * 3,
        ],
        compiler_params=pltpu.CompilerParams(
            collective_id=0, has_side_effects=True, vmem_limit_bytes=26 * 2**20
        ),
        cost_estimate=pl.CostEstimate(
            flops=2 * batch * elements,
            bytes_accessed=2 * elements + 4 * state.size,
            transcendentals=0,
        ),
        name="fused",
    )(
        rates,
        *[in_hbm(a) for a in (x, mg.reshape(1, block), cg.reshape(1, block))],
        *[in_hbm(a) for a in (qw, kw, vw, gw, ow, uw, dw, state)],
    )
    return pl.pallas_call(
        write_kernel,
        out_shape=[pltpu.HBM((batch, block), BF16), pltpu.HBM(state.shape, F32)],
        in_specs=[VM, VM],
        out_specs=[ANY, ANY],
        scratch_shapes=[DMA, DMA((seqs, CHUNKS))],
        compiler_params=pltpu.CompilerParams(vmem_limit_bytes=2**20),
        cost_estimate=pl.CostEstimate(
            flops=state.size, bytes_accessed=4 * state.size, transcendentals=0
        ),
        name="write",
    )(out, held)


def solution(mesh):
    return jax.shard_map(
        functools.partial(fused_device, mesh.shape["kv"], mesh.shape["tp"]),
        mesh=mesh,
        in_specs=(
            P(None, ("kv", "tp")),
            P(("kv", "tp")),
            P(("kv", "tp")),
            P("kv", "tp"),
            P("kv", "tp"),
            P("kv", "tp"),
            P("kv", "tp"),
            P("tp", "kv"),
            P("kv", "tp"),
            P("tp", "kv"),
            P("kv", "tp", None, None),
        ),
        out_specs=(P(None, ("kv", "tp")), P("kv", "tp", None, None)),
        check_vma=False,
    )
```

```python
import functools

import jax
import jax.numpy as jnp
from jax import lax
from jax.experimental import pallas as pl
from jax.experimental.pallas import tpu as pltpu
from jax.sharding import PartitionSpec as P

HEADS = 16
EPS = 1e-06
MESH = pl.DeviceIdType.MESH
F32 = jnp.float32
BF16 = jnp.bfloat16
DMA = pltpu.SemaphoreType.DMA
PAIR = 2
CORES = 2
GAIN_ROWS = 16
WIDTH = 512
LAG_A, LAG_B = 5, 5
LAG_1, LAG_2, LAG_3, LAG_4 = 4, 4, 4, 3
DIRECT_M, DIRECT_H = 2, 2
ALONG_A, ALONG_U = (3, 4), (3, 4)
SEND = (0, 3, 4, 1, 2)
FOLD = (0, 1, 2, 3, 5, 4)
HOLD, EARLY = 6, 2
CHUNKS = 1


def head_decays(count):
    index = jnp.arange(count, dtype=jnp.float32)
    return 1.0 - 2.0 ** (-1.0 - 6.0 * index / (count - 1))


def put(src, dst, send_sem, recv_sem, where):
    copy = pltpu.make_async_remote_copy(
        src_ref=src,
        dst_ref=dst,
        send_sem=send_sem,
        recv_sem=recv_sem,
        device_id=where,
        device_id_type=MESH,
    )
    copy.start()
    return copy


def landed(ref, sem):
    pltpu.make_async_copy(ref, ref, sem).wait()


def tp_gather(buf, tp, n_tp, sems):
    for d in range(1, n_tp):
        put(buf.at[tp], buf.at[tp], sems.at[0], sems.at[1], {"tp": lax.rem(tp + d, n_tp)})


def tp_scatter(src, dst, tp, n_tp, sems):
    for d in range(1, n_tp):
        peer = lax.rem(tp + d, n_tp)
        put(src.at[peer], dst.at[d - 1], sems.at[0], sems.at[1], {"tp": peer})


def square_total(squares, sq_src, sq_dst, kv, n_kv, rows, sems):
    for g in range(n_kv):
        sq_src[g] = jnp.broadcast_to(squares[g * rows : (g + 1) * rows], sq_src.shape[1:])
    for d in range(1, n_kv):
        peer = lax.rem(kv + d, n_kv)
        put(sq_src.at[peer], sq_dst.at[d - 1], sems.at[0], sems.at[1], {"kv": peer})

    def finish():
        landed(sq_dst, sems.at[1])
        total = sq_src[kv]
        for d in range(n_kv - 1):
            total = total + sq_dst[d]
        return total[:, :1]

    return finish


def in_order(order, s):
    return order[s] if s < len(order) else s


class PairScatter:
    def __init__(self, kv, n_kv, rows, along, bufs, sends, sem_a, sem_b):
        self.kv, self.n_kv, self.n_z = kv, n_kv, n_kv // PAIR
        self.z, self.y = lax.div(kv, PAIR), lax.rem(kv, PAIR)
        self.rows, self.other = rows, {"kv": self.z * PAIR + 1 - self.y}
        self.part, self.got, self.summed, self.got2, self.got_all, self.kept = bufs
        self.along = {p: i for i, p in enumerate(along) if p < self.got.shape[0]}
        self.sends, self.sem_a, self.sem_b = sends, sem_a, sem_b

    def start(self, p, value):
        rows = self.rows
        for z in range(self.n_z):
            for y in range(PAIR):
                at = (z * PAIR + y) * rows
                self.part[p, y, z] = value[at : at + rows].astype(BF16)
        if p in self.along:
            for d in range(1, self.n_z):
                peer = lax.rem(self.z + d, self.n_z)
                put(
                    self.part.at[p, :, peer],
                    self.got_all.at[self.along[p], pl.ds((d - 1) * PAIR, PAIR)],
                    self.sends.at[2],
                    self.sem_b.at[p],
                    {"kv": peer * PAIR + self.y},
                )
            return
        put(
            self.part.at[p, 1 - self.y],
            self.got.at[p],
            self.sends.at[0],
            self.sem_a.at[p],
            self.other,
        )

    def middle(self, p):
        if p in self.along:
            at, count = self.along[p], (self.n_z - 1) * PAIR
            landed(self.got_all.at[at, pl.ds(0, count)], self.sem_b.at[p])

            def total(y):
                value = self.part[p, y, self.z].astype(F32)
                for d in range(0, count, PAIR):
                    value = value + self.got_all[at, d + y].astype(F32)
                return value

            self.summed[p, 0] = total(1 - self.y).astype(BF16)
            self.kept[at] = total(self.y)
            put(
                self.summed.at[p, 0],
                self.got.at[p, 0],
                self.sends.at[3],
                self.sem_a.at[p],
                self.other,
            )
            return
        landed(self.got.at[p], self.sem_a.at[p])
        self.summed[p] = (self.part[p, self.y].astype(F32) + self.got[p].astype(F32)).astype(BF16)
        for d in range(1, self.n_z):
            peer = lax.rem(self.z + d, self.n_z)
            put(
                self.summed.at[p, peer],
                self.got2.at[p, d - 1],
                self.sends.at[1],
                self.sem_b.at[p],
                {"kv": peer * PAIR + self.y},
            )

    def finish(self, p):
        if p in self.along:
            landed(self.got.at[p, 0], self.sem_a.at[p])
            return self.kept[self.along[p]] + self.got[p, 0].astype(F32)
        landed(self.got2.at[p], self.sem_b.at[p])
        total = self.summed[p, self.z].astype(F32)
        for d in range(self.n_z - 1):
            total = total + self.got2[p, d].astype(F32)
        return total

    def drain(self):
        n = len(self.along)
        rest = pl.ds(0, self.got.shape[0] - n)
        landed(self.got.at[rest], self.sends.at[0])
        landed(self.got2.at[rest], self.sends.at[1])
        if n:
            blocks = self.got_all.at[pl.ds(0, n), pl.ds(0, (self.n_z - 1) * PAIR)]
            landed(blocks, self.sends.at[2])
            landed(self.got.at[pl.ds(0, n), 0], self.sends.at[3])


class PairGather:
    def __init__(self, kv, n_kv, direct, buf, like, sends, sem_z, sem_y):
        self.kv, self.n_kv, self.n_z = kv, n_kv, n_kv // PAIR
        self.z, self.y = lax.div(kv, PAIR), lax.rem(kv, PAIR)
        self.relayed, self.direct = buf.shape[0] - direct, direct
        self.buf, self.like = buf, like
        self.sends, self.sem_z, self.sem_y = sends, sem_z, sem_y

    def start(self, p):
        own = self.buf.at[p, self.z, self.y]
        if p >= self.relayed:
            for d in range(1, self.n_kv):
                peer = {"kv": lax.rem(self.kv + d, self.n_kv)}
                put(own, own, self.sends.at[2], self.sem_z.at[p], peer)
            return
        for d in range(1, self.n_z):
            peer = lax.rem(self.z + d, self.n_z)
            put(own, own, self.sends.at[0], self.sem_z.at[p], {"kv": peer * PAIR + self.y})

    def relay(self, p):
        if p >= self.relayed:
            return
        landed(self.buf.at[p, pl.ds(0, self.n_z - 1), 0], self.sem_z.at[p])
        put(
            self.buf.at[p, :, self.y],
            self.buf.at[p, :, self.y],
            self.sends.at[1],
            self.sem_y.at[p],
            {"kv": self.z * PAIR + 1 - self.y},
        )

    def finish(self, p):
        if p >= self.relayed:
            landed(self.like.at[0], self.sem_z.at[p])
        else:
            landed(self.buf.at[p, :, 0], self.sem_y.at[p])
        blocks = [
            self.buf[p, z, y].astype(F32) for z in range(self.n_z) for y in range(PAIR)
        ]
        return jnp.concatenate(blocks, axis=0).astype(BF16)

    def drain(self):
        rest = pl.ds(0, self.relayed)
        landed(self.buf.at[rest, pl.ds(0, self.n_z - 1), 0], self.sends.at[0])
        landed(self.buf.at[rest, :, 0], self.sends.at[1])
        if self.direct:
            landed(self.like.at[pl.ds(0, self.direct)], self.sends.at[2])


def fused_kernel(sizes, rate_ref, x_hbm, mg_hbm, cg_hbm, *refs):
    n_kv, n_tp, rows, width, dk, dv, heads, dim = sizes
    (qw_hbm, kw_hbm, vw_hbm, gw_hbm, ow_hbm, up_hbm, down_hbm, old_hbm) = refs[:8]
    (out_ref, held) = refs[8:10]
    (pack, gain_in, qw, kw, vw, gw, ow, up, down) = refs[10:19]
    bufs, bufs_u, refs = refs[19:25], refs[25:31], refs[31:]
    (sq_src, sq_dst, sq_src2, sq_dst2, mixes, hid, ret, acc, keys, vals) = refs[:10]
    (pair_own, pair_got, chip, far, mids, ends, got_ends) = refs[10:17]
    (w_sem, s_sem, in_sem, t_sem, sq_sem, sq_sem2) = refs[17:23]
    sems, sems_h = refs[23:26], refs[28:31]
    sems_u, sems_m = (refs[26], *sems[1:]), (refs[27], *sems_h[1:])
    (c_sem, far_sem, f_sem) = refs[31:34]
    kv, tp = lax.axis_index("kv"), lax.axis_index("tp")
    z, y = lax.div(kv, PAIR), lax.rem(kv, PAIR)
    n_x = n_tp // CORES
    cx, core = lax.div(tp, CORES), lax.rem(tp, CORES)
    batch, block = x_hbm.shape
    loads = {}

    def load(name, src, dst, sem):
        loads[name] = pltpu.make_async_copy(src, dst, sem)
        loads[name].start()

    barrier = pltpu.get_barrier_semaphore()
    for d in range(1, n_kv):
        pl.semaphore_signal(
            barrier, inc=1, device_id={"kv": lax.rem(kv + d, n_kv)}, device_id_type=MESH
        )
    for d in range(1, n_tp):
        pl.semaphore_signal(
            barrier, inc=1, device_id={"tp": lax.rem(tp + d, n_tp)}, device_id_type=MESH
        )
    load("x", x_hbm, pack.at[tp, pl.ds(0, batch)], in_sem.at[0])
    load("mg", mg_hbm, gain_in.at[0], in_sem.at[1])
    load("cg", cg_hbm, gain_in.at[1], in_sem.at[2])
    for name in ("x", "mg", "cg"):
        loads[name].wait()
    for i, (name, src, dst) in enumerate(
        [("q", qw_hbm, qw), ("k", kw_hbm, kw), ("v", vw_hbm, vw), ("g", gw_hbm, gw)]
    ):
        load(name, src, dst, w_sem.at[i])
    for i in range(2):
        gain = jnp.broadcast_to(gain_in[i].astype(F32), (GAIN_ROWS, block))
        pack[tp, batch + i * GAIN_ROWS : batch + (i + 1) * GAIN_ROWS] = gain.astype(BF16)
    pl.semaphore_wait(barrier, n_tp + n_kv - 2)
    tp_gather(pack, tp, n_tp, t_sem)
    load("old", old_hbm, held, s_sem)
    landed(pack.at[pl.ds(0, n_tp - 1)], t_sem.at[1])

    def normalise(stream, row):
        parts = [
            (stream[t] * pack[t, row : row + GAIN_ROWS][:1].astype(F32)).astype(BF16)
            for t in range(n_tp)
        ]
        return jnp.concatenate(parts, axis=1)

    def squares_of(stream):
        return sum(jnp.sum(s * s, axis=1, keepdims=True) for s in stream)

    stream = [pack[t, :batch].astype(F32) for t in range(n_tp)]
    normed = normalise(stream, batch)
    sq_total = square_total(squares_of(stream), sq_src, sq_dst, kv, n_kv, rows, sq_sem)
    scatter = PairScatter(kv, n_kv, rows, ALONG_A, bufs, *sems)
    mix_gather = PairGather(kv, n_kv, DIRECT_M, mixes, bufs[4], *sems_m)

    ready = set()

    def project(p):
        h, kind = divmod(p, 3)
        for name in (("q", "k"), ("v",), ("g",))[kind]:
            if name not in ready:
                loads[name].wait()
                ready.add(name)
        if kind == 0:
            cols = slice(h * dk, (h + 1) * dk)
            return jnp.concatenate(
                [
                    jnp.dot(normed, qw[:, cols], preferred_element_type=F32),
                    jnp.dot(normed, kw[:, cols], preferred_element_type=F32),
                ],
                axis=1,
            )
        w = (vw, gw)[kind - 1]
        return jnp.dot(normed, w[:, h * dv : (h + 1) * dv], preferred_element_type=F32)

    def retain(h, query, key, value):
        columns = query.T
        step = min(dk, 64)
        for s in range(rows):
            total = jnp.zeros((8, dv), F32)
            for r in range(0, dk, step):
                term = columns[r : r + step, s : s + 1] * held[s, h, r : r + step]
                total = total + jnp.sum(term.reshape(step // 8, 8, dv), axis=0)
            ret[s : s + 1] = jnp.sum(total, axis=0, keepdims=True)
        out = rate_ref[h] * ret[...] + jnp.sum(query * key, axis=1, keepdims=True) * value
        ret[...] = out * lax.rsqrt(jnp.mean(out * out, axis=1, keepdims=True) + EPS)

    def update(h):
        columns, value = keys[h].T, vals[h]
        step = min(dk, 64)
        for s in range(rows):
            line = value[s : s + 1]
            for r in range(0, dk, step):
                term = columns[r : r + step, s : s + 1] * line
                held[s, h, r : r + step] = rate_ref[h] * held[s, h, r : r + step] + term

    def attend(h):
        if h == 0:
            loads["ow"].wait()
        term = jnp.dot(
            mix_gather.finish(h), ow[h * dv : (h + 1) * dv], preferred_element_type=F32
        )
        acc[...] = term if h == 0 else acc[...] + term

    pieces = 3 * heads
    scale, values, pending = None, {}, []
    for s in range(pieces + LAG_A + LAG_B):
        if s < pieces:
            first = in_order(SEND, s)
            scatter.start(first, project(first))
        if s == 0:
            load("ow", ow_hbm, ow, w_sem.at[4])
            load("up", up_hbm, up, w_sem.at[5])
            load("down", down_hbm, down, w_sem.at[6])
        p = s - LAG_A
        if 0 <= p < pieces:
            scatter.middle(in_order(FOLD, p))
        p = p - LAG_B
        if 0 <= p < pieces:
            if p == 0:
                scale = lax.rsqrt(sq_total() / dim + EPS)
            h, kind = divmod(p, 3)
            total = scatter.finish(p) * scale
            if kind == 0:
                query, key = total[:, :dk], total[:, dk:] * dk ** (-0.5)
                keys[h] = key
                values["q"], values["k"] = query, key
            elif kind == 1:
                vals[h] = total
                if h == 0:
                    loads["old"].wait()
                retain(h, values["q"], values["k"], total)
            else:
                mixes[h, z, y] = (jax.nn.silu(total) * ret[...]).astype(BF16)
                if h < heads - 1:
                    pending.append(h)
                else:
                    mix_gather.start(h)
            if p >= HOLD:
                for g in pending:
                    mix_gather.start(g)
                pending = []
    for h in range(heads - 1):
        mix_gather.relay(h)
    for h in range(min(EARLY, heads - 1)):
        update(h)
    for h in range(heads):
        attend(h)

    half = pair_own.shape[1] // 2
    pair_own[...] = acc[...].astype(BF16)
    pair_copy = put(
        pair_own, pair_got, c_sem.at[0], c_sem.at[1], {"tp": cx * CORES + 1 - core}
    )
    pair_copy.wait_recv()
    both = pair_own[...].astype(F32) + pair_got[...].astype(F32)
    for j in range(CORES):
        chip[j] = both[:, j * half : (j + 1) * half].astype(BF16)
    for d in range(1, n_x):
        for rel in range(CORES):
            peer = lax.rem(cx + d, n_x) * CORES + lax.rem(core + rel, CORES)
            put(
                chip.at[core],
                far.at[d - 1, rel],
                far_sem.at[0],
                far_sem.at[1],
                {"tp": peer},
            )
    for h in range(min(EARLY, heads - 1), heads):
        update(h)
    landed(far, far_sem.at[1])
    sums = []
    for j in range(CORES):
        total = chip[j].astype(F32)
        for d in range(n_x - 1):
            total = total + far[d, lax.rem(core + j, CORES)].astype(F32)
        sums.append(total)
    attention = jnp.concatenate(sums, axis=1)
    for t in range(n_tp):
        mids[t] = (
            pack[t, :batch].astype(F32) + attention[:, t * block : (t + 1) * block]
        ).astype(BF16)
    stream = [mids[t].astype(F32) for t in range(n_tp)]
    normed_mid = normalise(stream, batch + GAIN_ROWS)
    sq_total2 = square_total(squares_of(stream), sq_src2, sq_dst2, kv, n_kv, rows, sq_sem2)
    lift = PairScatter(kv, n_kv, rows, ALONG_U, bufs_u, *sems_u)
    gather = PairGather(kv, n_kv, DIRECT_H, hid, bufs_u[4], *sems_h)
    count = up.shape[1] // width
    loads["up"].wait()
    scale2 = None
    for s in range(count + LAG_1 + LAG_2 + LAG_3 + LAG_4):
        if s < count:
            first = in_order(SEND if count > 5 else (), s)
            w = up[:, first * width : (first + 1) * width]
            lift.start(first, jnp.dot(normed_mid, w, preferred_element_type=F32))
        p = s - LAG_1
        if 0 <= p < count:
            lift.middle(in_order(FOLD if count > 5 else (), p))
        p = p - LAG_2
        if 0 <= p < count:
            if p == 0:
                scale2 = lax.rsqrt(sq_total2() / dim + EPS)
            lifted = lift.finish(p) * scale2
            hid[p, z, y] = jnp.square(jnp.maximum(lifted, 0.0)).astype(BF16)
            gather.start(p)
        p = p - LAG_3
        if 0 <= p < count:
            gather.relay(p)
        p = p - LAG_4
        if 0 <= p < count:
            if p == 0:
                loads["down"].wait()
            w = down[p * width : (p + 1) * width]
            term = jnp.dot(gather.finish(p), w, preferred_element_type=F32)
            acc[...] = term if p == 0 else acc[...] + term
    for t in range(n_tp):
        ends[t] = acc[:, t * block : (t + 1) * block].astype(BF16)
    tp_scatter(ends, got_ends, tp, n_tp, f_sem)
    landed(got_ends, f_sem.at[1])
    lowered = ends[tp].astype(F32)
    for d in range(n_tp - 1):
        lowered = lowered + got_ends[d].astype(F32)
    out_ref[...] = (mids[tp].astype(F32) + lowered).astype(BF16)
    for group in (scatter, mix_gather, lift, gather):
        group.drain()
    pair_copy.wait_send()
    landed(pack.at[pl.ds(0, n_tp - 1)], t_sem.at[0])
    landed(sq_dst, sq_sem.at[0])
    landed(sq_dst2, sq_sem2.at[0])
    landed(far, far_sem.at[0])
    landed(got_ends, f_sem.at[0])


def write_kernel(act_ref, state_ref, act_out, state_out, act_sem, sem):
    copies = [pltpu.make_async_copy(act_ref, act_out, act_sem)]
    for s in range(state_ref.shape[0]):
        for h in range(CHUNKS):
            n = state_ref.shape[1] // CHUNKS
            part = (s, pl.ds(h * n, n))
            copies.append(
                pltpu.make_async_copy(state_ref.at[part], state_out.at[part], sem.at[s, h])
            )
    for copy in copies:
        copy.start()
    for copy in copies:
        copy.wait()


def in_hbm(a):
    return pltpu.with_memory_space_constraint(a, pltpu.HBM)


VM = pl.BlockSpec(memory_space=pltpu.VMEM)
SM = pl.BlockSpec(memory_space=pltpu.SMEM)
ANY = pl.BlockSpec(memory_space=pltpu.HBM)


def scatter_scratch(count, n_kv, rows, width, direct):
    n_z = n_kv // PAIR
    return [
        pltpu.VMEM((count, PAIR, n_z, rows, width), BF16),
        pltpu.VMEM((count, n_z, rows, width), BF16),
        pltpu.VMEM((count, n_z, rows, width), BF16),
        pltpu.VMEM((count, n_z - 1, rows, width), BF16),
        pltpu.VMEM((max(direct, 1), n_kv - 1, rows, width), BF16),
        pltpu.VMEM((max(direct, 1), rows, width), F32),
    ]


def fused_device(n_kv, n_tp, x, mg, cg, qw, kw, vw, gw, ow, uw, dw, state):
    seqs, heads, dk, dv = state.shape
    batch, block = x.shape
    dim = block * n_kv * n_tp
    n_z, n_x = n_kv // PAIR, n_tp // CORES
    depth, cols = qw.shape[0], ow.shape[1]
    width = min(WIDTH, uw.shape[1])
    count, pieces = uw.shape[1] // width, 3 * heads
    rates = lax.dynamic_slice_in_dim(
        head_decays(HEADS), lax.axis_index("tp") * heads, heads, 0
    )
    elements = sum(w.size for w in (qw, kw, vw, gw, ow, uw, dw))
    out, held = pl.pallas_call(
        functools.partial(fused_kernel, (n_kv, n_tp, seqs, width, dk, dv, heads, dim)),
        out_shape=[
            jax.ShapeDtypeStruct((batch, block), BF16),
            pltpu.VMEM(state.shape, F32),
        ],
        in_specs=[SM] + [ANY] * 11,
        out_specs=[VM] * 2,
        scratch_shapes=[
            pltpu.VMEM((n_tp, batch + 2 * GAIN_ROWS, block), BF16),
            pltpu.VMEM((2, 1, block), BF16),
            *[pltpu.VMEM(w.shape, BF16) for w in (qw, kw, vw, gw, ow, uw, dw)],
            *scatter_scratch(pieces, n_kv, seqs, dv, max(len(ALONG_A), DIRECT_M)),
            *scatter_scratch(count, n_kv, seqs, width, max(len(ALONG_U), DIRECT_H)),
            pltpu.VMEM((n_kv, seqs, 128), F32),
            pltpu.VMEM((n_kv - 1, seqs, 128), F32),
            pltpu.VMEM((n_kv, seqs, 128), F32),
            pltpu.VMEM((n_kv - 1, seqs, 128), F32),
            pltpu.VMEM((heads, n_z, PAIR, seqs, dv), BF16),
            pltpu.VMEM((count, n_z, PAIR, seqs, width), BF16),
            pltpu.VMEM((seqs, dv), F32),
            pltpu.VMEM((batch, cols), F32),
            pltpu.VMEM((heads, seqs, dk), F32),
            pltpu.VMEM((heads, seqs, dv), F32),
            pltpu.VMEM((batch, cols), BF16),
            pltpu.VMEM((batch, cols), BF16),
            pltpu.VMEM((CORES, batch, cols // CORES), BF16),
            pltpu.VMEM((max(n_x - 1, 1), CORES, batch, cols // CORES), BF16),
            pltpu.VMEM((n_tp, batch, block), BF16),
            pltpu.VMEM((n_tp, batch, block), BF16),
            pltpu.VMEM((n_tp - 1, batch, block), BF16),
            DMA((7,)),
            DMA,
            DMA((3,)),
            *[DMA((2,))] * 3,
            *[DMA((4,)), *[DMA((max(pieces, count),))] * 2],
            DMA((4,)),
            DMA((3,)),
            *[DMA((3,)), *[DMA((max(heads, count),))] * 2],
            *[DMA((2,))] * 3,
        ],
        compiler_params=pltpu.CompilerParams(
            collective_id=0, has_side_effects=True, vmem_limit_bytes=26 * 2**20
        ),
        cost_estimate=pl.CostEstimate(
            flops=2 * batch * elements,
            bytes_accessed=2 * elements + 4 * state.size,
            transcendentals=0,
        ),
        name="fused",
    )(
        rates,
        *[in_hbm(a) for a in (x, mg.reshape(1, block), cg.reshape(1, block))],
        *[in_hbm(a) for a in (qw, kw, vw, gw, ow, uw, dw, state)],
    )
    return pl.pallas_call(
        write_kernel,
        out_shape=[pltpu.HBM((batch, block), BF16), pltpu.HBM(state.shape, F32)],
        in_specs=[VM, VM],
        out_specs=[ANY, ANY],
        scratch_shapes=[DMA, DMA((seqs, CHUNKS))],
        compiler_params=pltpu.CompilerParams(vmem_limit_bytes=2**20),
        cost_estimate=pl.CostEstimate(
            flops=state.size, bytes_accessed=4 * state.size, transcendentals=0
        ),
        name="write",
    )(out, held)


def solution(mesh):
    return jax.shard_map(
        functools.partial(fused_device, mesh.shape["kv"], mesh.shape["tp"]),
        mesh=mesh,
        in_specs=(
            P(None, ("kv", "tp")),
            P(("kv", "tp")),
            P(("kv", "tp")),
            P("kv", "tp"),
            P("kv", "tp"),
            P("kv", "tp"),
            P("kv", "tp"),
            P("tp", "kv"),
            P("kv", "tp"),
            P("tp", "kv"),
            P("kv", "tp", None, None),
        ),
        out_specs=(P(None, ("kv", "tp")), P("kv", "tp", None, None)),
        check_vma=False,
    )
```
